256 devices in a mesh: ra: 32 (over z, y), cb: 8 (over x, core).
Axes of the slice: x: 4, y: 4, z: 8, core: 2. Of those that a mesh axis runs over, the one named last changes fastest.
Arguments:
- stream: bfloat16 [64, 1024], P(None, 'ra'), may hold values from -24 to 24, as said below
- gain_first: float32 [1024], P('ra'), may hold values from 0.5 to 1.5
- up_first: float32 [1024, 4096], P('ra', 'cb'), may hold values from -0.1875 to 0.1875
- down_first: float32 [4096, 1024], P('cb', 'ra'), may hold values from -0.09375 to 0.09375
- gain_second: float32 [1024], P('ra'), may hold values from 0.5 to 1.5
- up_second: float32 [1024, 4096], P('ra', 'cb'), may hold values from -0.1875 to 0.1875
- down_second: float32 [4096, 1024], P('cb', 'ra'), may hold values from -0.09375 to 0.09375
Outputs:
- read: bfloat16 [64, 1024], P(None, 'ra')
The draws below stay inside these ranges and needn't reach their ends.
Inputs may be any that keep to these rules, and one draw needn't show every extreme that they name: stream is of order one, and in each token one aligned block of 32 features is four times larger than the rest.
All inputs are finite; a program needn't handle non-finite values.
Results may differ from the reference program's by a relative error of at most 0.025.
Values may be sent and summed in bfloat16 or wider, within the bound.
A program may use at most 64 MiB of HBM per device.

```python
import jax
import jax.numpy as jnp
from jax import lax

D = 1024
FF = 4096
TOKENS = 64
COLS_RA = 32


def draw_stream(key, part):
    key_base, key_block = jax.random.split(key)
    base = jnp.clip(jax.random.normal(key_base, (TOKENS, D), jnp.float32), -6.0, 6.0)
    chosen = jax.random.randint(key_block, (TOKENS, 1), 0, D // COLS_RA)
    column_block = jnp.arange(D, dtype=jnp.int32)[None, :] // COLS_RA
    boosted = jnp.where(column_block == chosen, 4.0, 1.0)
    return (base * boosted).astype(jnp.bfloat16)


def shard_levels(rng, shape, cuts, low, largest):
    level, own = 1.0, jax.random.fold_in(rng, 6)
    for axis_at, shards_of in cuts:
        draws = jnp.exp(jax.random.uniform(jax.random.fold_in(own, axis_at), (shards_of,), jnp.float32, low / len(cuts), largest / len(cuts)))
        level = level * jnp.repeat(draws, shape[axis_at] // shards_of).reshape([-1 if axis == axis_at else 1 for axis in range(len(shape))])
    return level


def normal_values(own_key, extent, width, most, shards=(), held_as=jnp.bfloat16):
    gain = shard_levels(own_key, extent, shards, -0.22, 0.18) if shards else 1.0
    result = jax.random.normal(own_key, extent, jnp.float32) * width * gain
    return jnp.minimum(jnp.maximum(result, -most), most).astype(held_as)


def setup_inputs(seed: int = 0) -> dict:
    arg_keys = jax.random.split(jax.random.key(seed), 8)
    return {
        "stream": draw_stream(jax.random.fold_in(arg_keys[7], 71), 0),
        "gain_first": jnp.clip(1.0 + 0.1 * jax.random.normal(arg_keys[1], (D,), jnp.float32), 0.5, 1.5),
        "up_first": normal_values(arg_keys[2], (D, FF), D ** -0.5, 0.1875, ((0, 32), (1, 8)), jnp.float32),
        "down_first": normal_values(arg_keys[3], (FF, D), FF ** -0.5, 0.09375, ((0, 8), (1, 32)), jnp.float32),
        "gain_second": jnp.clip(1.0 + 0.1 * jax.random.normal(arg_keys[4], (D,), jnp.float32), 0.5, 1.5),
        "up_second": normal_values(arg_keys[5], (D, FF), D ** -0.5, 0.1875, ((0, 32), (1, 8)), jnp.float32),
        "down_second": normal_values(arg_keys[6], (FF, D), FF ** -0.5, 0.09375, ((0, 8), (1, 32)), jnp.float32),
    }


EPS = 1e-06
RESIDUAL = 0.25

def sublayer(stream, norm_gain, w_up, w_down):
    floated = stream.astype(jnp.float32)
    squares = lax.optimization_barrier(jnp.sum(floated * floated, axis=1, keepdims=True))
    factor = jax.lax.rsqrt(squares / D + EPS)
    normed = (floated * factor * norm_gain.astype(jnp.float32)).astype(jnp.bfloat16)
    preact = jnp.dot(normed, w_up.astype(jnp.bfloat16), preferred_element_type=jnp.float32)
    activated = jnp.square(jax.nn.relu(preact)).astype(jnp.bfloat16)
    branch = jnp.dot(activated, w_down.astype(jnp.bfloat16), preferred_element_type=jnp.float32)
    return (RESIDUAL * floated + branch).astype(jnp.bfloat16)

def reference(stream, gain_first, up_first, down_first, gain_second, up_second, down_second):
    middle = sublayer(stream, gain_first, up_first, down_first)
    return sublayer(middle, gain_second, up_second, down_second)
```

```python
import functools

import jax
import jax.numpy as jnp
from jax import lax
from jax.experimental import pallas as pl
from jax.experimental.pallas import tpu as pltpu
from jax.sharding import PartitionSpec as P

NZ, NY, NX = 8, 4, 4
EPS = 1e-06
RESIDUAL = 0.25
LANES = 128
MESH = pl.DeviceIdType.MESH
F32 = jnp.float32
BF16 = jnp.bfloat16
NT = (((1,), (1,)), ((), ()))


def ring(offset, size):
    return min(offset, size - offset)


def farthest_first(offsets):
    return sorted(
        offsets, key=lambda o: (-(ring(o[0], NZ) + ring(o[1], NY) + ring(o[2], NX)), o))


ROW = farthest_first([(0, k, 0) for k in range(1, NY)])
COLUMN = farthest_first([(k, 0, 0) for k in range(1, NZ)])
PLANE = farthest_first([(0, j, k) for j in range(NY) for k in range(NX) if j or k])


def kernel(
    width,
    stream_hbm, gain1_hbm, up1_hbm, down1_hbm, gain2_hbm, up2_hbm, down2_hbm,
    out_ref,
    gain_v, up_v, down_v, stage, wall, ut, pre, sq, branch, fin, fin_in,
    load_sem, w_ss, w_rs, u_ss, u_rs, pre_ss, pre_rs, sq_ss, sq_rs, br_ss, br_rs,
    fin_ss, fin_rs, fin_ss0,
):
    ra = lax.axis_index("ra")
    cb = lax.axis_index("cb")
    z, y = lax.div(ra, NY), lax.rem(ra, NY)
    x, core = lax.div(cb, 2), lax.rem(cb, 2)
    here = y * NX + x
    tokens = ut.shape[-1]
    cols = ut.shape[1]

    def device(offset, at_core):
        dz, dy, dx = offset
        to_z = lax.rem(z + dz, NZ) if dz else z
        to_y = lax.rem(y + dy, NY) if dy else y
        to_x = lax.rem(x + dx, NX) if dx else x
        return {"ra": to_z * NY + to_y, "cb": to_x * 2 + at_core}

    def send(src, dst, ss, rs, offset, at_core):
        pltpu.make_async_remote_copy(
            src_ref=src, dst_ref=dst, send_sem=ss, recv_sem=rs,
            device_id=device(offset, at_core), device_id_type=MESH,
        ).start()

    def arrived(ref, rs):
        pltpu.make_async_copy(ref, ref, rs).wait()

    loads = [
        pltpu.make_async_copy(src, dst, load_sem.at[i])
        for i, (src, dst) in enumerate((
            (gain1_hbm, gain_v.at[0]),
            (up1_hbm, up_v.at[0]),
            (down1_hbm, down_v.at[0]),
            (gain2_hbm, gain_v.at[1]),
            (up2_hbm, up_v.at[1]),
            (down2_hbm, down_v.at[1]),
        ))
    ]
    load_u = pltpu.make_async_copy(stream_hbm, ut.at[y], load_sem.at[6])
    barrier = pltpu.get_barrier_semaphore()

    def hello(offset, at_core):
        pl.semaphore_signal(
            barrier, inc=1, device_id=device(offset, at_core), device_id_type=MESH)

    def place(which, layer):
        if which == 0:
            column = jnp.broadcast_to(gain_v[layer], (LANES, cols)).T[:, :1]
            rows = (up_v[layer] * column).astype(BF16)
        else:
            rows = down_v[layer].astype(BF16)
        for j in range(NY):
            stage[2 * layer + which, j] = rows[:, j * LANES:(j + 1) * LANES]

    def wait_weights(which, layer):
        if which == 0:
            loads[3 * layer].wait()
            loads[3 * layer + 1].wait()
        else:
            loads[3 * layer + 2].wait()

    loads[0].start()
    loads[1].start()

    @pl.when(core == 1)
    def _():
        load_u.start()
        for offset in COLUMN + PLANE:
            hello(offset, 1)
        for offset in [(0, 0, 0)] + PLANE:
            hello(offset, 0)
        for load in loads[2:]:
            load.start()
        wait_weights(0, 0)
        place(0, 0)
        wall[0, NY + y] = stage[0, y]
        load_u.wait()
        pl.semaphore_wait(barrier, len(COLUMN) + len(PLANE) + NX * NY)

        for offset in ROW:
            send(ut.at[y], ut.at[y], u_ss, u_rs, offset, 1)
        for m in range(4):
            which, layer = m % 2, m // 2
            if m:
                wait_weights(which, layer)
                place(which, layer)
                wall[m, NY + y] = stage[m, y]
            for offset in ROW:
                peer = lax.rem(y + offset[1], NY)
                send(stage.at[m, peer], wall.at[m, NY + y], w_ss.at[m], w_rs.at[m], offset, 1)

        arrived(ut.at[pl.ds(0, NY - 1)], u_rs)
        u_t = ut[...].reshape(NY * cols, tokens).astype(F32)
        floated = u_t.T
        scaled = floated
        result_t = None
        for layer in range(2):
            sq[layer, z] = jnp.sum(u_t * u_t, axis=0, keepdims=True)
            arrived(wall.at[2 * layer, pl.ds(0, 2 * NY - 1)], w_rs.at[2 * layer])
            lhs = floated.astype(BF16)
            for c in range(2):
                up = wall[2 * layer, c * NY:(c + 1) * NY].reshape(NY * cols, LANES)
                part = jnp.dot(lhs, up, preferred_element_type=F32)
                pre[layer, z, c] = part.astype(BF16)
            for offset in COLUMN:
                send(pre.at[layer, z], pre.at[layer, z], pre_ss.at[layer], pre_rs.at[layer], offset, 1)
            for offset in COLUMN:
                send(sq.at[layer, z], sq.at[layer, z], sq_ss.at[layer], sq_rs.at[layer], offset, 1)
            arrived(wall.at[2 * layer + 1, pl.ds(0, 2 * NY - 1)], w_rs.at[2 * layer + 1])
            if layer == 1:
                residual = u_t * (RESIDUAL / (NX * NY))

            arrived(pre.at[layer, pl.ds(0, NZ - 1)], pre_rs.at[layer])
            acts = []
            for c in range(2):
                total = pre[layer, 0, c].astype(F32)
                for j in range(1, NZ):
                    total += pre[layer, j, c].astype(F32)
                positive = jnp.maximum(total, 0.0)
                acts.append((positive * positive).astype(BF16))
            downs = [
                wall[2 * layer + 1, c * NY:(c + 1) * NY].reshape(NY * cols, LANES)
                for c in range(2)
            ]
            if layer == 0:
                out = sum(
                    lax.dot_general(a, w, NT, preferred_element_type=F32)
                    for a, w in zip(acts, downs))
                branch[here] = out.astype(BF16)
                for offset in PLANE:
                    send(branch.at[here], branch.at[here], br_ss, br_rs, offset, 1)
            arrived(sq.at[layer, pl.ds(0, NZ - 1)], sq_rs.at[layer])
            squares = sq[layer, 0]
            for j in range(1, NZ):
                squares += sq[layer, j]
            factor = 1.0 / (squares / width + EPS)
            if layer == 0:
                scale = jnp.broadcast_to(factor, (LANES, tokens)).T
                arrived(branch.at[pl.ds(0, NX * NY - 1)], br_rs)
                total = branch[0].astype(F32)
                for j in range(1, NX * NY):
                    total += branch[j].astype(F32)
                floated = (RESIDUAL * floated + total * scale).astype(BF16).astype(F32)
                u_t = floated.T
            else:
                out = sum(
                    lax.dot_general(w, a, NT, preferred_element_type=F32)
                    for a, w in zip(acts, downs))
                out = (out * factor + residual).astype(BF16)
                for j in range(NY):
                    fin[j] = out[j * cols:(j + 1) * cols]
                for offset in PLANE:
                    peer = lax.rem(y + offset[1], NY)
                    send(fin.at[peer], fin_in.at[here], fin_ss0, fin_rs, offset, 0)
                    send(fin.at[peer], fin_in.at[here], fin_ss, fin_rs, offset, 1)
                send(fin.at[y], fin_in.at[here], fin_ss0, fin_rs, (0, 0, 0), 0)
                fin_in[here] = fin[y]
        arrived(fin_in.at[pl.ds(0, NX * NY - 1)], fin_rs)

    @pl.when(core == 0)
    def _():
        for offset in [(0, 0, 0)] + PLANE:
            hello(offset, 1)
        for load in loads[2:]:
            load.start()
        wait_weights(0, 0)
        place(0, 0)
        pl.semaphore_wait(barrier, NX * NY)
        for m in range(4):
            which, layer = m % 2, m // 2
            if m:
                wait_weights(which, layer)
                place(which, layer)
            for offset in ROW + [(0, 0, 0)]:
                peer = lax.rem(y + offset[1], NY)
                send(stage.at[m, peer], wall.at[m, y], w_ss.at[m], w_rs.at[m], offset, 1)
        for m in range(4):
            arrived(stage.at[m], w_ss.at[m])
        arrived(fin_in, fin_rs)

    total = fin_in[0].astype(F32)
    for j in range(1, NX * NY):
        total += fin_in[j].astype(F32)
    out_ref[...] = total.astype(BF16)

    @pl.when(core == 1)
    def _():
        arrived(ut.at[pl.ds(0, NY - 1)], u_ss)
        for m in range(4):
            arrived(stage.at[m, pl.ds(0, NY - 1)], w_ss.at[m])
        for layer in range(2):
            arrived(pre.at[layer, pl.ds(0, NZ - 1)], pre_ss.at[layer])
            arrived(sq.at[layer, pl.ds(0, NZ - 1)], sq_ss.at[layer])
        arrived(branch.at[pl.ds(0, NX * NY - 1)], br_ss)
        arrived(fin_in.at[pl.ds(0, NX * NY - 1)], fin_ss)
        arrived(fin_in, fin_ss0)


def local(stream, gain_first, up_first, down_first, gain_second, up_second, down_second):
    tokens, cols = stream.shape
    hidden = up_first.shape[1]
    dma = pltpu.SemaphoreType.DMA
    out = pl.pallas_call(
        functools.partial(kernel, cols * NZ * NY),
        out_shape=jax.ShapeDtypeStruct((cols, tokens), BF16),
        in_specs=[pl.BlockSpec(memory_space=pl.ANY)] * 7,
        out_specs=pl.BlockSpec(memory_space=pltpu.VMEM),
        scratch_shapes=[
            pltpu.VMEM((2, 1, cols), F32),
            pltpu.VMEM((2, cols, hidden), F32),
            pltpu.VMEM((2, cols, hidden), F32),
            pltpu.VMEM((4, NY, cols, LANES), BF16),
            pltpu.VMEM((4, 2 * NY, cols, LANES), BF16),
            pltpu.VMEM((NY, cols, tokens), BF16),
            pltpu.VMEM((2, NZ, 2, tokens, LANES), BF16),
            pltpu.VMEM((2, NZ, 1, tokens), F32),
            pltpu.VMEM((NX * NY, tokens, LANES), BF16),
            pltpu.VMEM((NY, cols, tokens), BF16),
            pltpu.VMEM((NX * NY, cols, tokens), BF16),
            dma((7,)),
            dma((4,)), dma((4,)),
            dma, dma,
            dma((2,)), dma((2,)),
            dma((2,)), dma((2,)),
            dma, dma,
            dma, dma, dma,
        ],
        compiler_params=pltpu.CompilerParams(
            collective_id=0, has_side_effects=True
        ),
    )(
        stream.T, gain_first.reshape(1, cols), up_first, down_first.T,
        gain_second.reshape(1, cols), up_second, down_second.T,
    )
    return out.T


def solution(mesh):
    return jax.shard_map(
        local,
        mesh=mesh,
        in_specs=(
            P(None, "ra"),
            P("ra"),
            P("ra", "cb"),
            P("cb", "ra"),
            P("ra"),
            P("ra", "cb"),
            P("cb", "ra"),
        ),
        out_specs=P(None, "ra"),
        check_vma=False,
    )
```

```python
import functools

import jax
import jax.numpy as jnp
from jax import lax
from jax.experimental import pallas as pl
from jax.experimental.pallas import tpu as pltpu
from jax.sharding import PartitionSpec as P

NZ, NY, NX = 8, 4, 4
EPS = 1e-06
RESIDUAL = 0.25
LANES = 128
MESH = pl.DeviceIdType.MESH
F32 = jnp.float32
BF16 = jnp.bfloat16
NT = (((1,), (1,)), ((), ()))


def ring(offset, size):
    return min(offset, size - offset)


def farthest_first(offsets):
    return sorted(
        offsets, key=lambda o: (-(ring(o[0], NZ) + ring(o[1], NY) + ring(o[2], NX)), o))


ALONG_Y = farthest_first([(0, k, 0) for k in range(1, NY)])
ALONG_X = farthest_first([(0, 0, k) for k in range(1, NX)])
ALONG_Z = farthest_first([(k, 0, 0) for k in range(1, NZ)])
PLANE = farthest_first([(0, j, k) for j in range(NY) for k in range(NX) if j or k])
HERE = (0, 0, 0)


def kernel(
    width,
    stream_hbm, gain1_hbm, up1_hbm, down1_hbm, gain2_hbm, up2_hbm, down2_hbm,
    out_ref,
    gain_v, up_v, down_v, stage, wall, ut, rows_v, pre, sq, branch, fin,
    load_sem, w_ss, w_rs, u_ss, u_rs, pre_ss, pre_rs, sq_ss, sq_rs, br_ss, br_rs,
    fin_ss, fin_rs, fin_ss0, go, all_in,
):
    ra = lax.axis_index("ra")
    cb = lax.axis_index("cb")
    z, y = lax.div(ra, NY), lax.rem(ra, NY)
    x, core = lax.div(cb, 2), lax.rem(cb, 2)
    here = y * NX + x
    cols, tokens = ut.shape[1:]
    mine = tokens // NY
    half = wall.shape[-1]

    def device(offset, at_core):
        dz, dy, dx = offset
        to_z = lax.rem(z + dz, NZ) if dz else z
        to_y = lax.rem(y + dy, NY) if dy else y
        to_x = lax.rem(x + dx, NX) if dx else x
        return {"ra": to_z * NY + to_y, "cb": to_x * 2 + at_core}

    def send(src, dst, ss, rs, offset, at_core):
        pltpu.make_async_remote_copy(
            src_ref=src, dst_ref=dst, send_sem=ss, recv_sem=rs,
            device_id=device(offset, at_core), device_id_type=MESH,
        ).start()

    def arrived(ref, rs):
        pltpu.make_async_copy(ref, ref, rs).wait()

    def signal(sem, offset, at_core):
        pl.semaphore_signal(
            sem, inc=1, device_id=device(offset, at_core), device_id_type=MESH)

    loads = [
        pltpu.make_async_copy(src, dst, load_sem.at[i])
        for i, (src, dst) in enumerate((
            (gain1_hbm, gain_v.at[0]),
            (up1_hbm, up_v.at[0]),
            (down1_hbm, down_v.at[0]),
            (gain2_hbm, gain_v.at[1]),
            (up2_hbm, up_v.at[1]),
            (down2_hbm, down_v.at[1]),
        ))
    ]
    load_u = pltpu.make_async_copy(stream_hbm, ut.at[y], load_sem.at[6])
    barrier = pltpu.get_barrier_semaphore()

    def weight(m):
        layer = m // 2
        if m % 2 == 0:
            loads[3 * layer].wait()
            loads[3 * layer + 1].wait()
            column = jnp.broadcast_to(gain_v[layer], (LANES, cols)).T[:, :1]
            rows = (up_v[layer] * column).astype(BF16)
        else:
            loads[3 * layer + 2].wait()
            rows = down_v[layer].astype(BF16)
        for h in range(2):
            stage[m, h] = rows[:, h * half:(h + 1) * half]

    def share(m, slot, offsets):
        for h in range(2):
            for offset in offsets:
                send(stage.at[m, h], wall.at[m, h, slot], w_ss.at[m], w_rs.at[m, h], offset, 1)

    loads[0].start()
    loads[1].start()

    @pl.when(core == 1)
    def _():
        load_u.start()
        for offset in ALONG_Y:
            signal(barrier, offset, 1)
        for offset in ALONG_Z + ALONG_X:
            signal(barrier, offset, 0)
        for load in loads[2:]:
            load.start()
        weight(0)
        load_u.wait()
        pl.semaphore_wait(barrier, NY)
        signal(go, HERE, 0)

        for offset in ALONG_Y:
            send(ut.at[y], ut.at[y], u_ss, u_rs, offset, 1)
        for m in range(4):
            if m:
                weight(m)
            share(m, NY + y, ALONG_Y)
            for h in range(2):
                wall[m, h, NY + y] = stage[m, h]

        arrived(ut.at[pl.ds(0, NY - 1)], u_rs)
        rows_v[...] = ut[...].reshape(NY * cols, tokens).astype(F32).T
        floated = rows_v[pl.ds(pl.multiple_of(y * mine, mine), mine)]
        for layer in range(2):
            lhs = floated.astype(BF16)
            for h in range(2):
                arrived(wall.at[2 * layer, h, pl.ds(0, 2 * NY - 1)], w_rs.at[2 * layer, h])
                for c in range(2):
                    up = wall[2 * layer, h, c * NY:(c + 1) * NY].reshape(NY * cols, half)
                    part = jnp.dot(lhs, up, preferred_element_type=F32)
                    pre[layer, h, z, :, c * half:(c + 1) * half] = part.astype(BF16)
                if layer == 0 and h == 0:
                    pl.semaphore_wait(all_in, 1)
                for offset in ALONG_Z:
                    send(pre.at[layer, h, z], pre.at[layer, h, z],
                         pre_ss.at[layer], pre_rs.at[layer, h], offset, 1)
            sq[layer, z] = jnp.sum((floated * floated).T, axis=0, keepdims=True)
            for offset in ALONG_Z:
                send(sq.at[layer, z], sq.at[layer, z], sq_ss.at[layer], sq_rs.at[layer], offset, 1)
            for h in range(2):
                arrived(wall.at[2 * layer + 1, h, pl.ds(0, 2 * NY - 1)], w_rs.at[2 * layer + 1, h])

            total = jnp.zeros((mine, LANES), F32)
            for h in range(2):
                arrived(pre.at[layer, h, pl.ds(0, NZ - 1)], pre_rs.at[layer, h])
                if h == 1:
                    arrived(sq.at[layer, pl.ds(0, NZ - 1)], sq_rs.at[layer])
                preact = pre[layer, h, 0].astype(F32)
                for j in range(1, NZ):
                    preact += pre[layer, h, j].astype(F32)
                positive = jnp.maximum(preact, 0.0)
                act = (positive * positive).astype(BF16)
                for c in range(2):
                    down = wall[2 * layer + 1, h, c * NY:(c + 1) * NY].reshape(NY * cols, half)
                    total += lax.dot_general(
                        act[:, c * half:(c + 1) * half], down, NT, preferred_element_type=F32)
            squares = sq[layer, 0]
            for j in range(1, NZ):
                squares += sq[layer, j]
            factor = 1.0 / (squares / width + EPS)
            scale = jnp.broadcast_to(factor, (LANES, mine)).T

            if layer == 0:
                branch[x] = total.astype(BF16)
                for offset in ALONG_X:
                    send(branch.at[x], branch.at[x], br_ss, br_rs, offset, 1)
                arrived(branch.at[pl.ds(0, NX - 1)], br_rs)
                total = branch[0].astype(F32)
                for j in range(1, NX):
                    total += branch[j].astype(F32)
                floated = (RESIDUAL * floated + total * scale).astype(BF16).astype(F32)
            else:
                fin[here] = (total * scale + floated * (RESIDUAL / NX)).astype(BF16)
                for offset in PLANE:
                    send(fin.at[here], fin.at[here], fin_ss0, fin_rs, offset, 0)
                    send(fin.at[here], fin.at[here], fin_ss, fin_rs, offset, 1)
                send(fin.at[here], fin.at[here], fin_ss0, fin_rs, HERE, 0)
        arrived(fin.at[pl.ds(0, NX * NY - 1)], fin_rs)

    @pl.when(core == 0)
    def _():
        signal(barrier, HERE, 1)
        for load in loads[2:]:
            load.start()
        weight(0)
        pl.semaphore_wait(go, 1)
        for m in range(4):
            if m:
                weight(m)
            share(m, y, ALONG_Y + [HERE])
        pl.semaphore_wait(barrier, NZ - 1 + NX - 1)
        signal(all_in, HERE, 1)
        for m in range(4):
            arrived(wall.at[m, :, pl.ds(0, NY)], w_ss.at[m])
        arrived(fin, fin_rs)

    blocks = []
    for j in range(NY):
        total = fin[j * NX].astype(F32)
        for k in range(1, NX):
            total += fin[j * NX + k].astype(F32)
        blocks.append(total.astype(BF16))
    pick = (
        lax.broadcasted_iota(jnp.int32, (cols, LANES), 1)
        == lax.broadcasted_iota(jnp.int32, (cols, LANES), 0) + y * cols
    ).astype(F32).astype(BF16)
    out_ref[...] = lax.dot_general(
        pick, jnp.concatenate(blocks, axis=0), NT, preferred_element_type=F32).astype(BF16)

    @pl.when(core == 1)
    def _():
        arrived(ut.at[pl.ds(0, NY - 1)], u_ss)
        for m in range(4):
            arrived(wall.at[m, :, pl.ds(0, NY - 1)], w_ss.at[m])
        for layer in range(2):
            arrived(pre.at[layer, :, pl.ds(0, NZ - 1)], pre_ss.at[layer])
            arrived(sq.at[layer, pl.ds(0, NZ - 1)], sq_ss.at[layer])
        arrived(branch.at[pl.ds(0, NX - 1)], br_ss)
        arrived(fin.at[pl.ds(0, NX * NY - 1)], fin_ss)
        arrived(fin, fin_ss0)


def local(stream, gain_first, up_first, down_first, gain_second, up_second, down_second):
    tokens, cols = stream.shape
    hidden = up_first.shape[1]
    mine = tokens // NY
    half = hidden // 2
    dma = pltpu.SemaphoreType.DMA
    operands = [
        pltpu.with_memory_space_constraint(a, pltpu.HBM) for a in (
            stream.T, gain_first.reshape(1, cols), up_first, down_first.T,
            gain_second.reshape(1, cols), up_second, down_second.T)
    ]
    out = pl.pallas_call(
        functools.partial(kernel, cols * NZ * NY),
        out_shape=jax.ShapeDtypeStruct((cols, tokens), BF16),
        in_specs=[pl.BlockSpec(memory_space=pl.ANY)] * 7,
        out_specs=pl.BlockSpec(memory_space=pltpu.VMEM),
        scratch_shapes=[
            pltpu.VMEM((2, 1, cols), F32),
            pltpu.VMEM((2, cols, hidden), F32),
            pltpu.VMEM((2, cols, hidden), F32),
            pltpu.VMEM((4, 2, cols, half), BF16),
            pltpu.VMEM((4, 2, 2 * NY, cols, half), BF16),
            pltpu.VMEM((NY, cols, tokens), BF16),
            pltpu.VMEM((tokens, NY * cols), F32),
            pltpu.VMEM((2, 2, NZ, mine, 2 * half), BF16),
            pltpu.VMEM((2, NZ, 1, mine), F32),
            pltpu.VMEM((NX, mine, LANES), BF16),
            pltpu.VMEM((NX * NY, mine, LANES), BF16),
            dma((7,)),
            dma((4,)), dma((4, 2)),
            dma, dma,
            dma((2,)), dma((2, 2)),
            dma((2,)), dma((2,)),
            dma, dma,
            dma, dma, dma,
            pltpu.SemaphoreType.REGULAR, pltpu.SemaphoreType.REGULAR,
        ],
        compiler_params=pltpu.CompilerParams(
            collective_id=0, has_side_effects=True, vmem_limit_bytes=16 * 1024 * 1024,
        ),
    )(*operands)
    return out.T


def solution(mesh):
    return jax.shard_map(
        local,
        mesh=mesh,
        in_specs=(
            P(None, "ra"),
            P("ra"),
            P("ra", "cb"),
            P("cb", "ra"),
            P("ra"),
            P("ra", "cb"),
            P("cb", "ra"),
        ),
        out_specs=P(None, "ra"),
        check_vma=False,
    )
```

```python
import functools

import jax
import jax.numpy as jnp
from jax import lax
from jax.experimental import pallas as pl
from jax.experimental.pallas import tpu as pltpu
from jax.sharding import PartitionSpec as P

NZ, NY, NX = 8, 4, 4
EPS = 1e-06
RESIDUAL = 0.25
LANES = 128
MESH = pl.DeviceIdType.MESH
F32 = jnp.float32
BF16 = jnp.bfloat16
NT = (((1,), (1,)), ((), ()))


def ring(offset, size):
    return min(offset, size - offset)


def farthest_first(offsets):
    return sorted(
        offsets, key=lambda o: (-(ring(o[0], NZ) + ring(o[1], NY) + ring(o[2], NX)), o))


ALONG_Y = farthest_first([(0, k, 0) for k in range(1, NY)])
ALONG_X = farthest_first([(0, 0, k) for k in range(1, NX)])
ALONG_Z = farthest_first([(k, 0, 0) for k in range(1, NZ)])
PLANE = farthest_first([(0, j, k) for j in range(NY) for k in range(NX) if j or k])
HERE = (0, 0, 0)


def kernel(
    width,
    stream_hbm, gain1_hbm, up1_hbm, down1_hbm, gain2_hbm, up2_hbm, down2_hbm,
    out_ref,
    gain_v, up_v, down_v, stage, wall, given, got, ut, rows_v, pre, sq, branch, fin,
    load_sem, w_ss, w_rs, got_ss, got_rs, u_ss, u_rs, pre_ss, pre_rs, sq_ss, sq_rs,
    br_ss, br_rs, fin_ss, fin_rs, fin_ss0, go, all_in,
):
    ra = lax.axis_index("ra")
    cb = lax.axis_index("cb")
    z, y = lax.div(ra, NY), lax.rem(ra, NY)
    x, core = lax.div(cb, 2), lax.rem(cb, 2)
    here = y * NX + x
    cols, tokens = ut.shape[1:]
    mine = tokens // NY

    def device(offset, at_core):
        dz, dy, dx = offset
        to_z = lax.rem(z + dz, NZ) if dz else z
        to_y = lax.rem(y + dy, NY) if dy else y
        to_x = lax.rem(x + dx, NX) if dx else x
        return {"ra": to_z * NY + to_y, "cb": to_x * 2 + at_core}

    def send(src, dst, ss, rs, offset, at_core):
        pltpu.make_async_remote_copy(
            src_ref=src, dst_ref=dst, send_sem=ss, recv_sem=rs,
            device_id=device(offset, at_core), device_id_type=MESH,
        ).start()

    def arrived(ref, rs):
        pltpu.make_async_copy(ref, ref, rs).wait()

    def signal(sem, offset, at_core):
        pl.semaphore_signal(
            sem, inc=1, device_id=device(offset, at_core), device_id_type=MESH)

    loads = [
        pltpu.make_async_copy(src, dst, load_sem.at[i])
        for i, (src, dst) in enumerate((
            (gain1_hbm, gain_v.at[0]),
            (up1_hbm, up_v.at[0]),
            (down1_hbm, down_v.at[0]),
            (gain2_hbm, gain_v.at[1]),
            (up2_hbm, up_v.at[1]),
            (down2_hbm, down_v.at[1]),
        ))
    ]
    load_u = pltpu.make_async_copy(stream_hbm, ut.at[y], load_sem.at[6])
    barrier = pltpu.get_barrier_semaphore()

    def first_products():
        load_u.wait()
        loads[0].wait()
        scaled = (ut[y].astype(F32).T * gain_v[0]).astype(BF16)
        loads[1].wait()
        part = jnp.dot(scaled, up_v[0].astype(BF16), preferred_element_type=F32).astype(BF16)
        for j in range(NY):
            given[j] = part[j * mine:(j + 1) * mine]

    def share_products(c, offsets):
        for offset in offsets:
            peer = lax.rem(y + offset[1], NY)
            send(given.at[peer], got.at[c, y], got_ss, got_rs.at[c], offset, 1)

    def weight(m):
        if m == 1:
            loads[3].wait()
            loads[4].wait()
            column = jnp.broadcast_to(gain_v[1], (LANES, cols)).T[:, :1]
            stage[m] = (up_v[1] * column).astype(BF16)
        else:
            loads[2 if m == 0 else 5].wait()
            stage[m] = down_v[m // 2].astype(BF16)

    def share(m, slot, offsets):
        for offset in offsets:
            send(stage.at[m], wall.at[m, slot], w_ss.at[m], w_rs.at[m], offset, 1)

    def whole(m, c):
        return wall[m, c * NY:(c + 1) * NY].reshape(NY * cols, wall.shape[-1])

    loads[0].start()
    loads[1].start()
    load_u.start()

    @pl.when(core == 1)
    def _():
        for offset in ALONG_Y:
            signal(barrier, offset, 1)
        for offset in ALONG_Z + ALONG_X:
            signal(barrier, offset, 0)
        for load in loads[2:]:
            load.start()
        first_products()
        got[1, y] = given[y]
        pl.semaphore_wait(barrier, NY)
        signal(go, HERE, 0)

        share_products(1, ALONG_Y)
        for offset in ALONG_Y:
            send(ut.at[y], ut.at[y], u_ss, u_rs, offset, 1)
        for m in range(3):
            weight(m)
            share(m, NY + y, ALONG_Y)
            wall[m, NY + y] = stage[m]

        floated = None
        for layer in range(2):
            for c in (1, 0):
                if layer == 0:
                    arrived(got.at[c, pl.ds(0, NY - c)], got_rs.at[c])
                    part = got[c, 0].astype(F32)
                    for j in range(1, NY):
                        part += got[c, j].astype(F32)
                else:
                    if c:
                        arrived(wall.at[1, pl.ds(0, 2 * NY - 1)], w_rs.at[1])
                    part = jnp.dot(floated.astype(BF16), whole(1, c), preferred_element_type=F32)
                pre[layer, c, z] = part.astype(BF16)
                if layer == 0 and c:
                    pl.semaphore_wait(all_in, 1)
                for offset in ALONG_Z:
                    send(pre.at[layer, c, z], pre.at[layer, c, z],
                         pre_ss.at[layer], pre_rs.at[layer, c], offset, 1)
            if layer == 0:
                arrived(ut.at[pl.ds(0, NY - 1)], u_rs)
                rows_v[...] = ut[...].reshape(NY * cols, tokens).astype(F32).T
                floated = rows_v[pl.ds(pl.multiple_of(y * mine, mine), mine)]
            sq[layer, z] = jnp.sum((floated * floated).T, axis=0, keepdims=True)
            for offset in ALONG_Z:
                send(sq.at[layer, z], sq.at[layer, z], sq_ss.at[layer], sq_rs.at[layer], offset, 1)
            arrived(wall.at[2 * layer, pl.ds(0, 2 * NY - 1)], w_rs.at[2 * layer])

            total = jnp.zeros((mine, LANES), F32)
            for c in (1, 0):
                arrived(pre.at[layer, c, pl.ds(0, NZ - 1)], pre_rs.at[layer, c])
                if c == 0:
                    arrived(sq.at[layer, pl.ds(0, NZ - 1)], sq_rs.at[layer])
                preact = pre[layer, c, 0].astype(F32)
                for j in range(1, NZ):
                    preact += pre[layer, c, j].astype(F32)
                positive = jnp.maximum(preact, 0.0)
                act = (positive * positive).astype(BF16)
                total += lax.dot_general(
                    act, whole(2 * layer, c), NT, preferred_element_type=F32)
            squares = sq[layer, 0]
            for j in range(1, NZ):
                squares += sq[layer, j]
            factor = 1.0 / (squares / width + EPS)
            scale = jnp.broadcast_to(factor, (LANES, mine)).T

            if layer == 0:
                branch[x] = total.astype(BF16)
                for offset in ALONG_X:
                    send(branch.at[x], branch.at[x], br_ss, br_rs, offset, 1)
                arrived(branch.at[pl.ds(0, NX - 1)], br_rs)
                total = branch[0].astype(F32)
                for j in range(1, NX):
                    total += branch[j].astype(F32)
                floated = (RESIDUAL * floated + total * scale).astype(BF16).astype(F32)
            else:
                fin[here] = (total * scale + floated * (RESIDUAL / NX)).astype(BF16)
                for offset in PLANE:
                    send(fin.at[here], fin.at[here], fin_ss, fin_rs, offset, 1)
                for offset in PLANE + [HERE]:
                    send(fin.at[here], fin.at[here], fin_ss0, fin_rs, offset, 0)
        arrived(fin.at[pl.ds(0, NX * NY - 1)], fin_rs)

    @pl.when(core == 0)
    def _():
        signal(barrier, HERE, 1)
        for load in loads[2:]:
            load.start()
        first_products()
        pl.semaphore_wait(go, 1)
        share_products(0, ALONG_Y + [HERE])
        for m in range(3):
            weight(m)
            share(m, y, ALONG_Y + [HERE])
        pl.semaphore_wait(barrier, NZ - 1 + NX - 1)
        signal(all_in, HERE, 1)
        arrived(given, got_ss)
        for m in range(3):
            arrived(wall.at[m, pl.ds(0, NY)], w_ss.at[m])
        arrived(fin, fin_rs)

    blocks = []
    for j in range(NY):
        total = fin[j * NX].astype(F32)
        for k in range(1, NX):
            total += fin[j * NX + k].astype(F32)
        blocks.append(total.astype(BF16))
    pick = (
        lax.broadcasted_iota(jnp.int32, (cols, LANES), 1)
        == lax.broadcasted_iota(jnp.int32, (cols, LANES), 0) + y * cols
    ).astype(F32).astype(BF16)
    out_ref[...] = lax.dot_general(
        pick, jnp.concatenate(blocks, axis=0), NT, preferred_element_type=F32).astype(BF16)

    @pl.when(core == 1)
    def _():
        arrived(ut.at[pl.ds(0, NY - 1)], u_ss)
        arrived(given.at[pl.ds(0, NY - 1)], got_ss)
        for m in range(3):
            arrived(wall.at[m, pl.ds(0, NY - 1)], w_ss.at[m])
        for layer in range(2):
            arrived(pre.at[layer, :, pl.ds(0, NZ - 1)], pre_ss.at[layer])
            arrived(sq.at[layer, pl.ds(0, NZ - 1)], sq_ss.at[layer])
        arrived(branch.at[pl.ds(0, NX - 1)], br_ss)
        arrived(fin.at[pl.ds(0, NX * NY - 1)], fin_ss)
        arrived(fin, fin_ss0)


def local(stream, gain_first, up_first, down_first, gain_second, up_second, down_second):
    tokens, cols = stream.shape
    hidden = up_first.shape[1]
    mine = tokens // NY
    dma = pltpu.SemaphoreType.DMA
    operands = [
        pltpu.with_memory_space_constraint(a, pltpu.HBM) for a in (
            stream.T, gain_first.reshape(1, cols), up_first, down_first.T,
            gain_second.reshape(1, cols), up_second, down_second.T)
    ]
    out = pl.pallas_call(
        functools.partial(kernel, cols * NZ * NY),
        out_shape=jax.ShapeDtypeStruct((cols, tokens), BF16),
        in_specs=[pl.BlockSpec(memory_space=pl.ANY)] * 7,
        out_specs=pl.BlockSpec(memory_space=pltpu.VMEM),
        scratch_shapes=[
            pltpu.VMEM((2, 1, cols), F32),
            pltpu.VMEM((2, cols, hidden), F32),
            pltpu.VMEM((2, cols, hidden), F32),
            pltpu.VMEM((3, cols, hidden), BF16),
            pltpu.VMEM((3, 2 * NY, cols, hidden), BF16),
            pltpu.VMEM((NY, mine, hidden), BF16),
            pltpu.VMEM((2, NY, mine, hidden), BF16),
            pltpu.VMEM((NY, cols, tokens), BF16),
            pltpu.VMEM((tokens, NY * cols), F32),
            pltpu.VMEM((2, 2, NZ, mine, hidden), BF16),
            pltpu.VMEM((2, NZ, 1, mine), F32),
            pltpu.VMEM((NX, mine, LANES), BF16),
            pltpu.VMEM((NX * NY, mine, LANES), BF16),
            dma((7,)),
            dma((3,)), dma((3,)),
            dma, dma((2,)),
            dma, dma,
            dma((2,)), dma((2, 2)),
            dma((2,)), dma((2,)),
            dma, dma,
            dma, dma, dma,
            pltpu.SemaphoreType.REGULAR, pltpu.SemaphoreType.REGULAR,
        ],
        compiler_params=pltpu.CompilerParams(
            collective_id=0, has_side_effects=True, vmem_limit_bytes=16 * 1024 * 1024,
        ),
    )(*operands)
    return out.T


def solution(mesh):
    return jax.shard_map(
        local,
        mesh=mesh,
        in_specs=(
            P(None, "ra"),
            P("ra"),
            P("ra", "cb"),
            P("cb", "ra"),
            P("ra"),
            P("ra", "cb"),
            P("cb", "ra"),
        ),
        out_specs=P(None, "ra"),
        check_vma=False,
    )
```

```python
import functools

import jax
import jax.numpy as jnp
from jax import lax
from jax.experimental import pallas as pl
from jax.experimental.pallas import tpu as pltpu
from jax.sharding import PartitionSpec as P

NZ, NY, NX = 8, 4, 4
CHUNKS = 4
EPS = 1e-06
RESIDUAL = 0.25
LANES = 128
MESH = pl.DeviceIdType.MESH
F32 = jnp.float32
BF16 = jnp.bfloat16
NT = (((1,), (1,)), ((), ()))


def ring(offset, size):
    return min(offset, size - offset)


def farthest_first(offsets):
    return sorted(
        offsets, key=lambda o: (-(ring(o[0], NZ) + ring(o[1], NY) + ring(o[2], NX)), o))


ALONG_Y = farthest_first([(0, k, 0) for k in range(1, NY)])
ALONG_X = farthest_first([(0, 0, k) for k in range(1, NX)])
ALONG_Z = farthest_first([(k, 0, 0) for k in range(1, NZ)])
FAR, NEAR, MIXED = [4, 3, 5, 2, 6, 1, 7], [7, 1, 6, 2, 5, 3, 4], [1, 7, 4, 2, 6, 3, 5]
Z_ORDERS = [[FAR, FAR, FAR, FAR], [NEAR, NEAR, MIXED, MIXED]]
PLANE = farthest_first([(0, j, k) for j in range(NY) for k in range(NX) if j or k])
HERE = (0, 0, 0)


def kernel(
    width,
    stream_hbm, gain1_hbm, up1_hbm, down1_hbm, gain2_hbm, up2_hbm, down2_hbm,
    out_ref,
    gain_v, up_v, down_v, stage, wall, given, got, ut, rows_v, pre, sq, branch, fin,
    load_sem, w_ss, w_rs, got_ss, got_rs, u_ss, u_rs, pre_ss, pre_rs, sq_ss, sq_rs,
    br_ss, br_rs, fin_ss, fin_rs, fin_ss0, go, all_in,
):
    ra = lax.axis_index("ra")
    cb = lax.axis_index("cb")
    z, y = lax.div(ra, NY), lax.rem(ra, NY)
    x, core = lax.div(cb, 2), lax.rem(cb, 2)
    here = y * NX + x
    cols, tokens = ut.shape[1:]
    mine = tokens // NY

    def device(offset, at_core):
        dz, dy, dx = offset
        to_z = lax.rem(z + dz, NZ) if dz else z
        to_y = lax.rem(y + dy, NY) if dy else y
        to_x = lax.rem(x + dx, NX) if dx else x
        return {"ra": to_z * NY + to_y, "cb": to_x * 2 + at_core}

    def send(src, dst, ss, rs, offset, at_core):
        pltpu.make_async_remote_copy(
            src_ref=src, dst_ref=dst, send_sem=ss, recv_sem=rs,
            device_id=device(offset, at_core), device_id_type=MESH,
        ).start()

    def arrived(ref, rs):
        pltpu.make_async_copy(ref, ref, rs).wait()

    def signal(sem, offset, at_core):
        pl.semaphore_signal(
            sem, inc=1, device_id=device(offset, at_core), device_id_type=MESH)

    loads = [
        pltpu.make_async_copy(src, dst, load_sem.at[i])
        for i, (src, dst) in enumerate((
            (gain1_hbm, gain_v.at[0]),
            (up1_hbm, up_v.at[0]),
            (down1_hbm, down_v.at[0]),
            (gain2_hbm, gain_v.at[1]),
            (up2_hbm, up_v.at[1]),
            (down2_hbm, down_v.at[1]),
        ))
    ]
    load_u = pltpu.make_async_copy(stream_hbm, ut.at[y], load_sem.at[6])
    barrier = pltpu.get_barrier_semaphore()

    def first_products():
        load_u.wait()
        loads[0].wait()
        scaled = (ut[y].astype(F32).T * gain_v[0]).astype(BF16)
        loads[1].wait()
        part = jnp.dot(scaled, up_v[0].astype(BF16), preferred_element_type=F32).astype(BF16)
        for j in range(NY):
            given[j] = part[j * mine:(j + 1) * mine]

    def share_products(c, offsets):
        for offset in offsets:
            peer = lax.rem(y + offset[1], NY)
            send(given.at[peer], got.at[c, y], got_ss, got_rs.at[c], offset, 1)

    def weight(m):
        if m == 1:
            loads[3].wait()
            loads[4].wait()
            column = jnp.broadcast_to(gain_v[1], (LANES, cols)).T[:, :1]
            stage[m] = (up_v[1] * column).astype(BF16)
        else:
            loads[2 if m == 0 else 5].wait()
            stage[m] = down_v[m // 2].astype(BF16)

    def share(m, slot, offsets):
        for offset in offsets:
            send(stage.at[m], wall.at[m, slot], w_ss.at[m], w_rs.at[m], offset, 1)

    def whole(m, c):
        return wall[m, c * NY:(c + 1) * NY].reshape(NY * cols, wall.shape[-1])

    loads[0].start()
    loads[1].start()
    load_u.start()

    @pl.when(core == 1)
    def _():
        for offset in ALONG_Y:
            signal(barrier, offset, 1)
        for offset in ALONG_Z + ALONG_X:
            signal(barrier, offset, 0)
        for load in loads[2:]:
            load.start()
        first_products()
        got[1, y] = given[y]
        pl.semaphore_wait(barrier, NY)
        signal(go, HERE, 0)

        share_products(1, ALONG_Y)
        for offset in ALONG_Y:
            send(ut.at[y], ut.at[y], u_ss, u_rs, offset, 1)
        for m in range(3):
            weight(m)
            share(m, NY + y, ALONG_Y)
            wall[m, NY + y] = stage[m]

        def share_squares(layer, u):
            sq[layer, z] = jnp.sum((u * u).T, axis=0, keepdims=True)
            for offset in ALONG_Z:
                send(sq.at[layer, z], sq.at[layer, z], sq_ss.at[layer], sq_rs.at[layer], offset, 1)

        floated = None
        wide = pre.shape[-1]
        for layer in range(2):
            for q in range(CHUNKS):
                c, lane = 1 - q // (CHUNKS // 2), q % (CHUNKS // 2) * wide
                if layer == 0 and not lane:
                    arrived(got.at[c, pl.ds(0, NY - c)], got_rs.at[c])
                    part = got[c, 0].astype(F32)
                    for j in range(1, NY):
                        part += got[c, j].astype(F32)
                elif not lane:
                    if c:
                        arrived(wall.at[1, pl.ds(0, 2 * NY - 1)], w_rs.at[1])
                    part = jnp.dot(floated.astype(BF16), whole(1, c), preferred_element_type=F32)
                pre[layer, q, z] = part[:, lane:lane + wide].astype(BF16)
                if layer == 0 and q == 0:
                    pl.semaphore_wait(all_in, 1)
                for k in Z_ORDERS[layer][q]:
                    send(pre.at[layer, q, z], pre.at[layer, q, z],
                         pre_ss.at[layer], pre_rs.at[layer, q], (k, 0, 0), 1)
                if layer == 1 and q == 0:
                    share_squares(1, floated)
            if layer == 0:
                arrived(ut.at[pl.ds(0, NY - 1)], u_rs)
                rows_v[...] = ut[...].reshape(NY * cols, tokens).astype(F32).T
                floated = rows_v[pl.ds(pl.multiple_of(y * mine, mine), mine)]
                share_squares(0, floated)
            arrived(wall.at[2 * layer, pl.ds(0, 2 * NY - 1)], w_rs.at[2 * layer])

            total = jnp.zeros((mine, LANES), F32)
            for q in range(CHUNKS):
                c, lane = 1 - q // (CHUNKS // 2), q % (CHUNKS // 2) * wide
                arrived(pre.at[layer, q, pl.ds(0, NZ - 1)], pre_rs.at[layer, q])
                preact = pre[layer, q, 0].astype(F32)
                for j in range(1, NZ):
                    preact += pre[layer, q, j].astype(F32)
                positive = jnp.maximum(preact, 0.0)
                act = (positive * positive).astype(BF16)
                total += lax.dot_general(
                    act, whole(2 * layer, c)[:, lane:lane + wide], NT, preferred_element_type=F32)
            if layer == 0:
                branch[x] = total.astype(BF16)
                for offset in ALONG_X:
                    send(branch.at[x], branch.at[x], br_ss, br_rs, offset, 1)
            arrived(sq.at[layer, pl.ds(0, NZ - 1)], sq_rs.at[layer])
            squares = sq[layer, 0]
            for j in range(1, NZ):
                squares += sq[layer, j]
            factor = 1.0 / (squares / width + EPS)
            scale = jnp.broadcast_to(factor, (LANES, mine)).T

            if layer == 0:
                arrived(branch.at[pl.ds(0, NX - 1)], br_rs)
                total = branch[0].astype(F32)
                for j in range(1, NX):
                    total += branch[j].astype(F32)
                floated = (RESIDUAL * floated + total * scale).astype(BF16).astype(F32)
            else:
                fin[here] = (total * scale + floated * (RESIDUAL / NX)).astype(BF16)
                for offset in PLANE:
                    send(fin.at[here], fin.at[here], fin_ss, fin_rs, offset, 1)
                for offset in PLANE + [HERE]:
                    send(fin.at[here], fin.at[here], fin_ss0, fin_rs, offset, 0)
        arrived(fin.at[pl.ds(0, NX * NY - 1)], fin_rs)

    @pl.when(core == 0)
    def _():
        signal(barrier, HERE, 1)
        for load in loads[2:]:
            load.start()
        first_products()
        pl.semaphore_wait(go, 1)
        share_products(0, ALONG_Y + [HERE])
        for m in range(3):
            weight(m)
            share(m, y, ALONG_Y + [HERE])
        pl.semaphore_wait(barrier, NZ - 1 + NX - 1)
        signal(all_in, HERE, 1)
        arrived(given, got_ss)
        for m in range(3):
            arrived(wall.at[m, pl.ds(0, NY)], w_ss.at[m])
        arrived(fin, fin_rs)

    blocks = []
    for j in range(NY):
        total = fin[j * NX].astype(F32)
        for k in range(1, NX):
            total += fin[j * NX + k].astype(F32)
        blocks.append(total.astype(BF16))
    pick = (
        lax.broadcasted_iota(jnp.int32, (cols, LANES), 1)
        == lax.broadcasted_iota(jnp.int32, (cols, LANES), 0) + y * cols
    ).astype(F32).astype(BF16)
    out_ref[...] = lax.dot_general(
        pick, jnp.concatenate(blocks, axis=0), NT, preferred_element_type=F32).astype(BF16)

    @pl.when(core == 1)
    def _():
        arrived(ut.at[pl.ds(0, NY - 1)], u_ss)
        arrived(given.at[pl.ds(0, NY - 1)], got_ss)
        for m in range(3):
            arrived(wall.at[m, pl.ds(0, NY - 1)], w_ss.at[m])
        for layer in range(2):
            arrived(pre.at[layer, :, pl.ds(0, NZ - 1)], pre_ss.at[layer])
            arrived(sq.at[layer, pl.ds(0, NZ - 1)], sq_ss.at[layer])
        arrived(branch.at[pl.ds(0, NX - 1)], br_ss)
        arrived(fin.at[pl.ds(0, NX * NY - 1)], fin_ss)
        arrived(fin, fin_ss0)


def local(stream, gain_first, up_first, down_first, gain_second, up_second, down_second):
    tokens, cols = stream.shape
    hidden = up_first.shape[1]
    mine = tokens // NY
    dma = pltpu.SemaphoreType.DMA
    operands = [
        pltpu.with_memory_space_constraint(a, pltpu.HBM) for a in (
            stream.T, gain_first.reshape(1, cols), up_first, down_first.T,
            gain_second.reshape(1, cols), up_second, down_second.T)
    ]
    out = pl.pallas_call(
        functools.partial(kernel, cols * NZ * NY),
        out_shape=jax.ShapeDtypeStruct((cols, tokens), BF16),
        in_specs=[pl.BlockSpec(memory_space=pl.ANY)] * 7,
        out_specs=pl.BlockSpec(memory_space=pltpu.VMEM),
        scratch_shapes=[
            pltpu.VMEM((2, 1, cols), F32),
            pltpu.VMEM((2, cols, hidden), F32),
            pltpu.VMEM((2, cols, hidden), F32),
            pltpu.VMEM((3, cols, hidden), BF16),
            pltpu.VMEM((3, 2 * NY, cols, hidden), BF16),
            pltpu.VMEM((NY, mine, hidden), BF16),
            pltpu.VMEM((2, NY, mine, hidden), BF16),
            pltpu.VMEM((NY, cols, tokens), BF16),
            pltpu.VMEM((tokens, NY * cols), F32),
            pltpu.VMEM((2, CHUNKS, NZ, mine, 2 * hidden // CHUNKS), BF16),
            pltpu.VMEM((2, NZ, 1, mine), F32),
            pltpu.VMEM((NX, mine, LANES), BF16),
            pltpu.VMEM((NX * NY, mine, LANES), BF16),
            dma((7,)),
            dma((3,)), dma((3,)),
            dma, dma((2,)),
            dma, dma,
            dma((2,)), dma((2, CHUNKS)),
            dma((2,)), dma((2,)),
            dma, dma,
            dma, dma, dma,
            pltpu.SemaphoreType.REGULAR, pltpu.SemaphoreType.REGULAR,
        ],
        compiler_params=pltpu.CompilerParams(
            collective_id=0, has_side_effects=True, vmem_limit_bytes=16 * 1024 * 1024,
        ),
    )(*operands)
    return out.T


def solution(mesh):
    return jax.shard_map(
        local,
        mesh=mesh,
        in_specs=(
            P(None, "ra"),
            P("ra"),
            P("ra", "cb"),
            P("cb", "ra"),
            P("ra"),
            P("ra", "cb"),
            P("cb", "ra"),
        ),
        out_specs=P(None, "ra"),
        check_vma=False,
    )
```

```python
import functools

import jax
import jax.numpy as jnp
from jax import lax
from jax.experimental import pallas as pl
from jax.experimental.pallas import tpu as pltpu
from jax.sharding import PartitionSpec as P

NZ, NY, NX = 8, 4, 4
CHUNKS = 4
EPS = 1e-06
RESIDUAL = 0.25
LANES = 128
MESH = pl.DeviceIdType.MESH
F32 = jnp.float32
BF16 = jnp.bfloat16
NT = (((1,), (1,)), ((), ()))


def ring(offset, size):
    return min(offset, size - offset)


def farthest_first(offsets):
    return sorted(
        offsets, key=lambda o: (-(ring(o[0], NZ) + ring(o[1], NY) + ring(o[2], NX)), o))


ALONG_Y = farthest_first([(0, k, 0) for k in range(1, NY)])
ALONG_X = farthest_first([(0, 0, k) for k in range(1, NX)])
ALONG_Z = farthest_first([(k, 0, 0) for k in range(1, NZ)])
LATER_Z = [1, 7, 2, 6, 3, 5, 4]
PLANE = farthest_first([(0, j, k) for j in range(NY) for k in range(NX) if j or k])
HERE = (0, 0, 0)


def kernel(
    width,
    stream_hbm, gain1_hbm, up1_hbm, down1_hbm, gain2_hbm, up2_hbm, down2_hbm,
    out_ref,
    gain_v, up_v, down_v, stage, wall, given, got, ut, rows_v, pre, sq, branch, fin,
    load_sem, w_ss, w_rs, got_ss, got_rs, u_ss, u_rs, pre_ss, pre_rs, sq_ss, sq_rs,
    br_ss, br_rs, fin_ss, fin_rs, fin_ss0, go, all_in, first_ss,
):
    ra = lax.axis_index("ra")
    cb = lax.axis_index("cb")
    z, y = lax.div(ra, NY), lax.rem(ra, NY)
    x, core = lax.div(cb, 2), lax.rem(cb, 2)
    here = y * NX + x
    cols, tokens = ut.shape[1:]
    mine = tokens // NY

    def device(offset, at_core):
        dz, dy, dx = offset
        to_z = lax.rem(z + dz, NZ) if dz else z
        to_y = lax.rem(y + dy, NY) if dy else y
        to_x = lax.rem(x + dx, NX) if dx else x
        return {"ra": to_z * NY + to_y, "cb": to_x * 2 + at_core}

    def send(src, dst, ss, rs, offset, at_core):
        pltpu.make_async_remote_copy(
            src_ref=src, dst_ref=dst, send_sem=ss, recv_sem=rs,
            device_id=device(offset, at_core), device_id_type=MESH,
        ).start()

    def arrived(ref, rs):
        pltpu.make_async_copy(ref, ref, rs).wait()

    def signal(sem, offset, at_core):
        pl.semaphore_signal(
            sem, inc=1, device_id=device(offset, at_core), device_id_type=MESH)

    loads = [
        pltpu.make_async_copy(src, dst, load_sem.at[i])
        for i, (src, dst) in enumerate((
            (gain1_hbm, gain_v.at[0]),
            (up1_hbm, up_v.at[0]),
            (down1_hbm, down_v.at[0]),
            (gain2_hbm, gain_v.at[1]),
            (up2_hbm, up_v.at[1]),
            (down2_hbm, down_v.at[1]),
        ))
    ]
    load_u = pltpu.make_async_copy(stream_hbm, ut.at[y], load_sem.at[6])
    barrier = pltpu.get_barrier_semaphore()

    def first_products():
        load_u.wait()
        loads[0].wait()
        scaled = (ut[y].astype(F32).T * gain_v[0]).astype(BF16)
        loads[1].wait()
        part = jnp.dot(scaled, up_v[0].astype(BF16), preferred_element_type=F32).astype(BF16)
        for j in range(NY):
            given[j] = part[j * mine:(j + 1) * mine]

    def share_products(c, offsets):
        for offset in offsets:
            peer = lax.rem(y + offset[1], NY)
            send(given.at[peer], got.at[c, y], got_ss, got_rs.at[c], offset, 1)

    def weight(m):
        if m == 1:
            loads[3].wait()
            loads[4].wait()
            column = jnp.broadcast_to(gain_v[1], (LANES, cols)).T[:, :1]
            stage[m] = (up_v[1] * column).astype(BF16)
        else:
            loads[2 if m == 0 else 5].wait()
            stage[m] = down_v[m // 2].astype(BF16)

    def share(m, slot, offsets):
        for offset in offsets:
            send(stage.at[m], wall.at[m, slot], w_ss.at[m], w_rs.at[m], offset, 1)

    def whole(m, c):
        return wall[m, c * NY:(c + 1) * NY].reshape(NY * cols, wall.shape[-1])

    loads[0].start()
    loads[1].start()
    load_u.start()

    @pl.when(core == 1)
    def _():
        for offset in ALONG_Y:
            signal(barrier, offset, 1)
        for offset in ALONG_Z + ALONG_X:
            signal(barrier, offset, 0)
        for load in loads[2:]:
            load.start()
        first_products()
        got[1, y] = given[y]
        pl.semaphore_wait(barrier, NY)
        signal(go, HERE, 0)

        share_products(1, ALONG_Y)
        for offset in ALONG_Y:
            send(ut.at[y], ut.at[y], u_ss, u_rs, offset, 1)
        for m in range(3):
            weight(m)
            share(m, NY + y, ALONG_Y)
            wall[m, NY + y] = stage[m]

        def send_second(to_z, q, ss):
            @pl.when(z != to_z)
            def _():
                pltpu.make_async_remote_copy(
                    src_ref=pre.at[1, q, z], dst_ref=pre.at[1, q, z],
                    send_sem=ss, recv_sem=pre_rs.at[1, q],
                    device_id={"ra": to_z * NY + y, "cb": x * 2 + 1}, device_id_type=MESH,
                ).start()

        def sent_second(to_z, ss):
            @pl.when(z != to_z)
            def _():
                arrived(pre.at[1, :, 0], ss)

        def share_squares(layer, u):
            sq[layer, z] = jnp.sum((u * u).T, axis=0, keepdims=True)
            for offset in ALONG_Z:
                send(sq.at[layer, z], sq.at[layer, z], sq_ss.at[layer], sq_rs.at[layer], offset, 1)

        floated = None
        wide = pre.shape[-1]
        for layer in range(2):
            for q in range(CHUNKS):
                c, lane = 1 - q // (CHUNKS // 2), q % (CHUNKS // 2) * wide
                if layer == 0 and not lane:
                    arrived(got.at[c, pl.ds(0, NY - c)], got_rs.at[c])
                    part = got[c, 0].astype(F32)
                    for j in range(1, NY):
                        part += got[c, j].astype(F32)
                elif not lane:
                    if c:
                        arrived(wall.at[1, pl.ds(0, 2 * NY - 1)], w_rs.at[1])
                    part = jnp.dot(floated.astype(BF16), whole(1, c), preferred_element_type=F32)
                pre[layer, q, z] = part[:, lane:lane + wide].astype(BF16)
                if layer == 0 and q == 0:
                    pl.semaphore_wait(all_in, 1)
                if layer == 0:
                    for offset in ALONG_Z:
                        send(pre.at[0, q, z], pre.at[0, q, z],
                             pre_ss.at[0], pre_rs.at[0, q], offset, 1)
                else:
                    send_second(0, q, first_ss)
                if layer == 1 and q == 0:
                    share_squares(1, floated)
            if layer == 1:
                sent_second(0, first_ss)
                for to_z in LATER_Z:
                    for q in range(CHUNKS):
                        send_second(to_z, q, pre_ss.at[1])
            else:
                arrived(ut.at[pl.ds(0, NY - 1)], u_rs)
                rows_v[...] = ut[...].reshape(NY * cols, tokens).astype(F32).T
                floated = rows_v[pl.ds(pl.multiple_of(y * mine, mine), mine)]
                share_squares(0, floated)
            arrived(wall.at[2 * layer, pl.ds(0, 2 * NY - 1)], w_rs.at[2 * layer])

            def scale_of(layer):
                arrived(sq.at[layer, pl.ds(0, NZ - 1)], sq_rs.at[layer])
                squares = sq[layer, 0]
                for j in range(1, NZ):
                    squares += sq[layer, j]
                factor = 1.0 / (squares / width + EPS)
                return jnp.broadcast_to(factor, (LANES, mine)).T

            total = jnp.zeros((mine, LANES), F32)
            for q in range(CHUNKS):
                c, lane = 1 - q // (CHUNKS // 2), q % (CHUNKS // 2) * wide
                if layer == 1 and q == CHUNKS - 1:
                    scale = scale_of(1)
                arrived(pre.at[layer, q, pl.ds(0, NZ - 1)], pre_rs.at[layer, q])
                preact = pre[layer, q, 0].astype(F32)
                for j in range(1, NZ):
                    preact += pre[layer, q, j].astype(F32)
                positive = jnp.maximum(preact, 0.0)
                act = (positive * positive).astype(BF16)
                total += lax.dot_general(
                    act, whole(2 * layer, c)[:, lane:lane + wide], NT, preferred_element_type=F32)
            if layer == 0:
                branch[x] = total.astype(BF16)
                for offset in ALONG_X:
                    send(branch.at[x], branch.at[x], br_ss, br_rs, offset, 1)
                scale = scale_of(0)

            if layer == 0:
                arrived(branch.at[pl.ds(0, NX - 1)], br_rs)
                total = branch[0].astype(F32)
                for j in range(1, NX):
                    total += branch[j].astype(F32)
                floated = (RESIDUAL * floated + total * scale).astype(BF16).astype(F32)
            else:
                fin[here] = (total * scale + floated * (RESIDUAL / NX)).astype(BF16)
                for offset in PLANE:
                    send(fin.at[here], fin.at[here], fin_ss, fin_rs, offset, 1)
                for offset in PLANE + [HERE]:
                    send(fin.at[here], fin.at[here], fin_ss0, fin_rs, offset, 0)
        arrived(fin.at[pl.ds(0, NX * NY - 1)], fin_rs)

    @pl.when(core == 0)
    def _():
        signal(barrier, HERE, 1)
        for load in loads[2:]:
            load.start()
        first_products()
        pl.semaphore_wait(go, 1)
        share_products(0, ALONG_Y + [HERE])
        for m in range(3):
            weight(m)
            share(m, y, ALONG_Y + [HERE])
        pl.semaphore_wait(barrier, NZ - 1 + NX - 1)
        signal(all_in, HERE, 1)
        arrived(given, got_ss)
        for m in range(3):
            arrived(wall.at[m, pl.ds(0, NY)], w_ss.at[m])
        arrived(fin, fin_rs)

    blocks = []
    for j in range(NY):
        total = fin[j * NX].astype(F32)
        for k in range(1, NX):
            total += fin[j * NX + k].astype(F32)
        blocks.append(total.astype(BF16))
    pick = (
        lax.broadcasted_iota(jnp.int32, (cols, LANES), 1)
        == lax.broadcasted_iota(jnp.int32, (cols, LANES), 0) + y * cols
    ).astype(F32).astype(BF16)
    out_ref[...] = lax.dot_general(
        pick, jnp.concatenate(blocks, axis=0), NT, preferred_element_type=F32).astype(BF16)

    @pl.when(core == 1)
    def _():
        arrived(ut.at[pl.ds(0, NY - 1)], u_ss)
        arrived(given.at[pl.ds(0, NY - 1)], got_ss)
        for m in range(3):
            arrived(wall.at[m, pl.ds(0, NY - 1)], w_ss.at[m])
        arrived(pre.at[0, :, pl.ds(0, NZ - 1)], pre_ss.at[0])
        for to_z in LATER_Z:
            @pl.when(z != to_z)
            def _():
                arrived(pre.at[1, :, 0], pre_ss.at[1])
        for layer in range(2):
            arrived(sq.at[layer, pl.ds(0, NZ - 1)], sq_ss.at[layer])
        arrived(branch.at[pl.ds(0, NX - 1)], br_ss)
        arrived(fin.at[pl.ds(0, NX * NY - 1)], fin_ss)
        arrived(fin, fin_ss0)


def local(stream, gain_first, up_first, down_first, gain_second, up_second, down_second):
    tokens, cols = stream.shape
    hidden = up_first.shape[1]
    mine = tokens // NY
    dma = pltpu.SemaphoreType.DMA
    operands = [
        pltpu.with_memory_space_constraint(a, pltpu.HBM) for a in (
            stream.T, gain_first.reshape(1, cols), up_first, down_first.T,
            gain_second.reshape(1, cols), up_second, down_second.T)
    ]
    out = pl.pallas_call(
        functools.partial(kernel, cols * NZ * NY),
        out_shape=jax.ShapeDtypeStruct((cols, tokens), BF16),
        in_specs=[pl.BlockSpec(memory_space=pl.ANY)] * 7,
        out_specs=pl.BlockSpec(memory_space=pltpu.VMEM),
        scratch_shapes=[
            pltpu.VMEM((2, 1, cols), F32),
            pltpu.VMEM((2, cols, hidden), F32),
            pltpu.VMEM((2, cols, hidden), F32),
            pltpu.VMEM((3, cols, hidden), BF16),
            pltpu.VMEM((3, 2 * NY, cols, hidden), BF16),
            pltpu.VMEM((NY, mine, hidden), BF16),
            pltpu.VMEM((2, NY, mine, hidden), BF16),
            pltpu.VMEM((NY, cols, tokens), BF16),
            pltpu.VMEM((tokens, NY * cols), F32),
            pltpu.VMEM((2, CHUNKS, NZ, mine, 2 * hidden // CHUNKS), BF16),
            pltpu.VMEM((2, NZ, 1, mine), F32),
            pltpu.VMEM((NX, mine, LANES), BF16),
            pltpu.VMEM((NX * NY, mine, LANES), BF16),
            dma((7,)),
            dma((3,)), dma((3,)),
            dma, dma((2,)),
            dma, dma,
            dma((2,)), dma((2, CHUNKS)),
            dma((2,)), dma((2,)),
            dma, dma,
            dma, dma, dma,
            pltpu.SemaphoreType.REGULAR, pltpu.SemaphoreType.REGULAR, dma,
        ],
        compiler_params=pltpu.CompilerParams(
            collective_id=0, has_side_effects=True, vmem_limit_bytes=16 * 1024 * 1024,
        ),
    )(*operands)
    return out.T


def solution(mesh):
    return jax.shard_map(
        local,
        mesh=mesh,
        in_specs=(
            P(None, "ra"),
            P("ra"),
            P("ra", "cb"),
            P("cb", "ra"),
            P("ra"),
            P("ra", "cb"),
            P("cb", "ra"),
        ),
        out_specs=P(None, "ra"),
        check_vma=False,
    )
```

```python
import functools

import jax
import jax.numpy as jnp
from jax import lax
from jax.experimental import pallas as pl
from jax.experimental.pallas import tpu as pltpu
from jax.sharding import PartitionSpec as P

NZ, NY, NX = 8, 4, 4
CHUNKS = 4
EPS = 1e-06
RESIDUAL = 0.25
LANES = 128
MESH = pl.DeviceIdType.MESH
F32 = jnp.float32
BF16 = jnp.bfloat16
NT = (((1,), (1,)), ((), ()))


def ring(offset, size):
    return min(offset, size - offset)


def farthest_first(offsets):
    return sorted(
        offsets, key=lambda o: (-(ring(o[0], NZ) + ring(o[1], NY) + ring(o[2], NX)), o))


ALONG_Y = farthest_first([(0, k, 0) for k in range(1, NY)])
ALONG_X = farthest_first([(0, 0, k) for k in range(1, NX)])
ALONG_Z = farthest_first([(k, 0, 0) for k in range(1, NZ)])
FIRST_Z = [[4, 3, 5, 2, 6, 1, 7], [3, 5, 2, 4, 6, 1, 7], [4, 5, 3, 2, 6, 1, 7], [4, 3, 5, 2, 6, 1, 7]]
LATER_Z = [1, 2, 7, 6, 3, 4, 5]
PLANE = farthest_first([(0, j, k) for j in range(NY) for k in range(NX) if j or k])
HERE = (0, 0, 0)


def kernel(
    width,
    stream_hbm, gain1_hbm, up1_hbm, down1_hbm, gain2_hbm, up2_hbm, down2_hbm,
    out_ref,
    gain_v, up_v, down_v, stage, wall, given, got, ut, rows_v, pre, sq, branch, fin,
    load_sem, w_ss, w_rs, got_ss, got_rs, u_ss, u_rs, pre_ss, pre_rs, sq_ss, sq_rs,
    br_ss, br_rs, fin_ss, fin_rs, fin_ss0, go, all_in, first_ss,
):
    ra = lax.axis_index("ra")
    cb = lax.axis_index("cb")
    z, y = lax.div(ra, NY), lax.rem(ra, NY)
    x, core = lax.div(cb, 2), lax.rem(cb, 2)
    here = y * NX + x
    cols, tokens = ut.shape[1:]
    mine = tokens // NY

    def device(offset, at_core):
        dz, dy, dx = offset
        to_z = lax.rem(z + dz, NZ) if dz else z
        to_y = lax.rem(y + dy, NY) if dy else y
        to_x = lax.rem(x + dx, NX) if dx else x
        return {"ra": to_z * NY + to_y, "cb": to_x * 2 + at_core}

    def send(src, dst, ss, rs, offset, at_core):
        pltpu.make_async_remote_copy(
            src_ref=src, dst_ref=dst, send_sem=ss, recv_sem=rs,
            device_id=device(offset, at_core), device_id_type=MESH,
        ).start()

    def arrived(ref, rs):
        pltpu.make_async_copy(ref, ref, rs).wait()

    def signal(sem, offset, at_core):
        pl.semaphore_signal(
            sem, inc=1, device_id=device(offset, at_core), device_id_type=MESH)

    loads = [
        pltpu.make_async_copy(src, dst, load_sem.at[i])
        for i, (src, dst) in enumerate((
            (gain1_hbm, gain_v.at[0]),
            (up1_hbm, up_v.at[0]),
            (down1_hbm, down_v.at[0]),
            (gain2_hbm, gain_v.at[1]),
            (up2_hbm, up_v.at[1]),
            (down2_hbm, down_v.at[1]),
        ))
    ]
    load_u = pltpu.make_async_copy(stream_hbm, ut.at[y], load_sem.at[6])
    barrier = pltpu.get_barrier_semaphore()

    def first_products():
        load_u.wait()
        loads[0].wait()
        scaled = (ut[y].astype(F32).T * gain_v[0]).astype(BF16)
        loads[1].wait()
        part = jnp.dot(scaled, up_v[0].astype(BF16), preferred_element_type=F32).astype(BF16)
        for j in range(NY):
            given[j] = part[j * mine:(j + 1) * mine]

    def share_products(c, offsets):
        for offset in offsets:
            peer = lax.rem(y + offset[1], NY)
            send(given.at[peer], got.at[c, y], got_ss, got_rs.at[c], offset, 1)

    def weight(m):
        if m == 1:
            loads[3].wait()
            loads[4].wait()
            column = jnp.broadcast_to(gain_v[1], (LANES, cols)).T[:, :1]
            stage[m] = (up_v[1] * column).astype(BF16)
        else:
            loads[2 if m == 0 else 5].wait()
            stage[m] = down_v[m // 2].astype(BF16)

    def share(m, slot, offsets):
        for offset in offsets:
            send(stage.at[m], wall.at[m, slot], w_ss.at[m], w_rs.at[m], offset, 1)

    def whole(m, c):
        return wall[m, c * NY:(c + 1) * NY].reshape(NY * cols, wall.shape[-1])

    loads[0].start()
    loads[1].start()
    load_u.start()

    @pl.when(core == 1)
    def _():
        for offset in ALONG_Y:
            signal(barrier, offset, 1)
        for offset in ALONG_Z + ALONG_X:
            signal(barrier, offset, 0)
        for load in loads[2:]:
            load.start()
        first_products()
        got[1, y] = given[y]
        pl.semaphore_wait(barrier, NY)
        signal(go, HERE, 0)

        share_products(1, ALONG_Y)
        for offset in ALONG_Y:
            send(ut.at[y], ut.at[y], u_ss, u_rs, offset, 1)
        for m in range(3):
            weight(m)
            share(m, NY + y, ALONG_Y)
            wall[m, NY + y] = stage[m]

        def send_second(to_z, q, ss):
            @pl.when(z != to_z)
            def _():
                pltpu.make_async_remote_copy(
                    src_ref=pre.at[1, q, z], dst_ref=pre.at[1, q, z],
                    send_sem=ss, recv_sem=pre_rs.at[1, q],
                    device_id={"ra": to_z * NY + y, "cb": x * 2 + 1}, device_id_type=MESH,
                ).start()

        def sent_second(to_z, ss):
            @pl.when(z != to_z)
            def _():
                arrived(pre.at[1, :, 0], ss)

        def share_squares(layer, u):
            sq[layer, z] = jnp.sum((u * u).T, axis=0, keepdims=True)
            for offset in ALONG_Z:
                send(sq.at[layer, z], sq.at[layer, z], sq_ss.at[layer], sq_rs.at[layer], offset, 1)

        floated = None
        wide = pre.shape[-1]
        for layer in range(2):
            for q in range(CHUNKS):
                c, lane = 1 - q // (CHUNKS // 2), q % (CHUNKS // 2) * wide
                if layer == 0 and not lane:
                    arrived(got.at[c, pl.ds(0, NY - c)], got_rs.at[c])
                    part = got[c, 0].astype(F32)
                    for j in range(1, NY):
                        part += got[c, j].astype(F32)
                elif not lane:
                    if c:
                        arrived(wall.at[1, pl.ds(0, 2 * NY - 1)], w_rs.at[1])
                    part = jnp.dot(floated.astype(BF16), whole(1, c), preferred_element_type=F32)
                pre[layer, q, z] = part[:, lane:lane + wide].astype(BF16)
                if layer == 0 and q == 0:
                    pl.semaphore_wait(all_in, 1)
                if layer == 0:
                    for k in FIRST_Z[q]:
                        send(pre.at[0, q, z], pre.at[0, q, z],
                             pre_ss.at[0], pre_rs.at[0, q], (k, 0, 0), 1)
                else:
                    send_second(0, q, first_ss)
                if layer == 1 and q == 0:
                    share_squares(1, floated)
            if layer == 1:
                sent_second(0, first_ss)
                for to_z in LATER_Z:
                    for q in range(CHUNKS):
                        send_second(to_z, q, pre_ss.at[1])
            else:
                arrived(ut.at[pl.ds(0, NY - 1)], u_rs)
                rows_v[...] = ut[...].reshape(NY * cols, tokens).astype(F32).T
                floated = rows_v[pl.ds(pl.multiple_of(y * mine, mine), mine)]
                share_squares(0, floated)
            arrived(wall.at[2 * layer, pl.ds(0, 2 * NY - 1)], w_rs.at[2 * layer])

            def scale_of(layer):
                arrived(sq.at[layer, pl.ds(0, NZ - 1)], sq_rs.at[layer])
                squares = sq[layer, 0]
                for j in range(1, NZ):
                    squares += sq[layer, j]
                factor = 1.0 / (squares / width + EPS)
                return jnp.broadcast_to(factor, (LANES, mine)).T

            total = jnp.zeros((mine, LANES), F32)
            for q in range(CHUNKS):
                c, lane = 1 - q // (CHUNKS // 2), q % (CHUNKS // 2) * wide
                if layer == 1 and q == CHUNKS - 1:
                    scale = scale_of(1)
                arrived(pre.at[layer, q, pl.ds(0, NZ - 1)], pre_rs.at[layer, q])
                preact = pre[layer, q, 0].astype(F32)
                for j in range(1, NZ):
                    preact += pre[layer, q, j].astype(F32)
                positive = jnp.maximum(preact, 0.0)
                act = (positive * positive).astype(BF16)
                total += lax.dot_general(
                    act, whole(2 * layer, c)[:, lane:lane + wide], NT, preferred_element_type=F32)
            if layer == 0:
                branch[x] = total.astype(BF16)
                for offset in ALONG_X:
                    send(branch.at[x], branch.at[x], br_ss, br_rs, offset, 1)
                scale = scale_of(0)

            if layer == 0:
                arrived(branch.at[pl.ds(0, NX - 1)], br_rs)
                total = branch[0].astype(F32)
                for j in range(1, NX):
                    total += branch[j].astype(F32)
                floated = (RESIDUAL * floated + total * scale).astype(BF16).astype(F32)
            else:
                fin[here] = (total * scale + floated * (RESIDUAL / NX)).astype(BF16)
                for offset in PLANE:
                    send(fin.at[here], fin.at[here], fin_ss, fin_rs, offset, 1)
                for offset in PLANE + [HERE]:
                    send(fin.at[here], fin.at[here], fin_ss0, fin_rs, offset, 0)
        arrived(fin.at[pl.ds(0, NX * NY - 1)], fin_rs)

    @pl.when(core == 0)
    def _():
        signal(barrier, HERE, 1)
        for load in loads[2:]:
            load.start()
        first_products()
        pl.semaphore_wait(go, 1)
        share_products(0, ALONG_Y + [HERE])
        for m in range(3):
            weight(m)
            share(m, y, ALONG_Y + [HERE])
        pl.semaphore_wait(barrier, NZ - 1 + NX - 1)
        signal(all_in, HERE, 1)
        arrived(given, got_ss)
        for m in range(3):
            arrived(wall.at[m, pl.ds(0, NY)], w_ss.at[m])
        arrived(fin, fin_rs)

    blocks = []
    for j in range(NY):
        total = fin[j * NX].astype(F32)
        for k in range(1, NX):
            total += fin[j * NX + k].astype(F32)
        blocks.append(total.astype(BF16))
    pick = (
        lax.broadcasted_iota(jnp.int32, (cols, LANES), 1)
        == lax.broadcasted_iota(jnp.int32, (cols, LANES), 0) + y * cols
    ).astype(F32).astype(BF16)
    out_ref[...] = lax.dot_general(
        pick, jnp.concatenate(blocks, axis=0), NT, preferred_element_type=F32).astype(BF16)

    @pl.when(core == 1)
    def _():
        arrived(ut.at[pl.ds(0, NY - 1)], u_ss)
        arrived(given.at[pl.ds(0, NY - 1)], got_ss)
        for m in range(3):
            arrived(wall.at[m, pl.ds(0, NY - 1)], w_ss.at[m])
        arrived(pre.at[0, :, pl.ds(0, NZ - 1)], pre_ss.at[0])
        for to_z in LATER_Z:
            @pl.when(z != to_z)
            def _():
                arrived(pre.at[1, :, 0], pre_ss.at[1])
        for layer in range(2):
            arrived(sq.at[layer, pl.ds(0, NZ - 1)], sq_ss.at[layer])
        arrived(branch.at[pl.ds(0, NX - 1)], br_ss)
        arrived(fin.at[pl.ds(0, NX * NY - 1)], fin_ss)
        arrived(fin, fin_ss0)


def local(stream, gain_first, up_first, down_first, gain_second, up_second, down_second):
    tokens, cols = stream.shape
    hidden = up_first.shape[1]
    mine = tokens // NY
    dma = pltpu.SemaphoreType.DMA
    operands = [
        pltpu.with_memory_space_constraint(a, pltpu.HBM) for a in (
            stream.T, gain_first.reshape(1, cols), up_first, down_first.T,
            gain_second.reshape(1, cols), up_second, down_second.T)
    ]
    out = pl.pallas_call(
        functools.partial(kernel, cols * NZ * NY),
        out_shape=jax.ShapeDtypeStruct((cols, tokens), BF16),
        in_specs=[pl.BlockSpec(memory_space=pl.ANY)] * 7,
        out_specs=pl.BlockSpec(memory_space=pltpu.VMEM),
        scratch_shapes=[
            pltpu.VMEM((2, 1, cols), F32),
            pltpu.VMEM((2, cols, hidden), F32),
            pltpu.VMEM((2, cols, hidden), F32),
            pltpu.VMEM((3, cols, hidden), BF16),
            pltpu.VMEM((3, 2 * NY, cols, hidden), BF16),
            pltpu.VMEM((NY, mine, hidden), BF16),
            pltpu.VMEM((2, NY, mine, hidden), BF16),
            pltpu.VMEM((NY, cols, tokens), BF16),
            pltpu.VMEM((tokens, NY * cols), F32),
            pltpu.VMEM((2, CHUNKS, NZ, mine, 2 * hidden // CHUNKS), BF16),
            pltpu.VMEM((2, NZ, 1, mine), F32),
            pltpu.VMEM((NX, mine, LANES), BF16),
            pltpu.VMEM((NX * NY, mine, LANES), BF16),
            dma((7,)),
            dma((3,)), dma((3,)),
            dma, dma((2,)),
            dma, dma,
            dma((2,)), dma((2, CHUNKS)),
            dma((2,)), dma((2,)),
            dma, dma,
            dma, dma, dma,
            pltpu.SemaphoreType.REGULAR, pltpu.SemaphoreType.REGULAR, dma,
        ],
        compiler_params=pltpu.CompilerParams(
            collective_id=0, has_side_effects=True, vmem_limit_bytes=16 * 1024 * 1024,
        ),
    )(*operands)
    return out.T


def solution(mesh):
    return jax.shard_map(
        local,
        mesh=mesh,
        in_specs=(
            P(None, "ra"),
            P("ra"),
            P("ra", "cb"),
            P("cb", "ra"),
            P("ra"),
            P("ra", "cb"),
            P("cb", "ra"),
        ),
        out_specs=P(None, "ra"),
        check_vma=False,
    )
```

```python
import functools

import jax
import jax.numpy as jnp
from jax import lax
from jax.experimental import pallas as pl
from jax.experimental.pallas import tpu as pltpu
from jax.sharding import PartitionSpec as P

NZ, NY, NX = 8, 4, 4
CHUNKS = 4
EPS = 1e-06
RESIDUAL = 0.25
LANES = 128
MESH = pl.DeviceIdType.MESH
F32 = jnp.float32
BF16 = jnp.bfloat16
NT = (((1,), (1,)), ((), ()))


def ring(offset, size):
    return min(offset, size - offset)


def farthest_first(offsets):
    return sorted(
        offsets, key=lambda o: (-(ring(o[0], NZ) + ring(o[1], NY) + ring(o[2], NX)), o))


ALONG_Y = farthest_first([(0, k, 0) for k in range(1, NY)])
ALONG_X = farthest_first([(0, 0, k) for k in range(1, NX)])
ALONG_Z = farthest_first([(k, 0, 0) for k in range(1, NZ)])
FIRST_Z = [[4, 3, 5, 2, 6, 1, 7], [3, 5, 2, 4, 6, 1, 7], [4, 5, 3, 2, 6, 1, 7], [4, 3, 5, 2, 6, 1, 7]]
LATER_Z = [1, 2, 7, 6, 3, 4, 5]
PLANE = farthest_first([(0, j, k) for j in range(NY) for k in range(NX) if j or k])
HERE = (0, 0, 0)


def kernel(
    width,
    stream_hbm, gain1_hbm, up1_hbm, down1_hbm, gain2_hbm, up2_hbm, down2_hbm,
    out_ref,
    gain_v, up_v, down_v, stage, wall, given, got, ut, rows_v, pre, sq, branch, fin,
    load_sem, w_ss, w_rs, got_ss, got_rs, u_ss, u_rs, pre_ss, pre_rs, sq_ss, sq_rs,
    br_ss, br_rs, fin_ss, fin_rs, fin_ss0, go, all_in, first_ss,
):
    ra = lax.axis_index("ra")
    cb = lax.axis_index("cb")
    z, y = lax.div(ra, NY), lax.rem(ra, NY)
    x, core = lax.div(cb, 2), lax.rem(cb, 2)
    here = y * NX + x
    cols, tokens = ut.shape[1:]
    mine = tokens // NY

    def device(offset, at_core):
        dz, dy, dx = offset
        to_z = lax.rem(z + dz, NZ) if dz else z
        to_y = lax.rem(y + dy, NY) if dy else y
        to_x = lax.rem(x + dx, NX) if dx else x
        return {"ra": to_z * NY + to_y, "cb": to_x * 2 + at_core}

    def send(src, dst, ss, rs, offset, at_core):
        pltpu.make_async_remote_copy(
            src_ref=src, dst_ref=dst, send_sem=ss, recv_sem=rs,
            device_id=device(offset, at_core), device_id_type=MESH,
        ).start()

    def arrived(ref, rs):
        pltpu.make_async_copy(ref, ref, rs).wait()

    def signal(sem, offset, at_core):
        pl.semaphore_signal(
            sem, inc=1, device_id=device(offset, at_core), device_id_type=MESH)

    loads = [
        pltpu.make_async_copy(src, dst, load_sem.at[i])
        for i, (src, dst) in enumerate((
            (gain1_hbm, gain_v.at[0]),
            (up1_hbm, up_v.at[0]),
            (down1_hbm, down_v.at[0]),
            (gain2_hbm, gain_v.at[1]),
            (up2_hbm, up_v.at[1]),
            (down2_hbm, down_v.at[1]),
        ))
    ]
    load_u = pltpu.make_async_copy(stream_hbm, ut.at[y], load_sem.at[6])
    barrier = pltpu.get_barrier_semaphore()

    def first_products():
        load_u.wait()
        loads[0].wait()
        scaled = (ut[y].astype(F32).T * gain_v[0]).astype(BF16)
        loads[1].wait()
        part = jnp.dot(scaled, up_v[0].astype(BF16), preferred_element_type=F32).astype(BF16)
        for j in range(NY):
            given[j] = part[j * mine:(j + 1) * mine]

    def share_products(c, offsets):
        for offset in offsets:
            peer = lax.rem(y + offset[1], NY)
            send(given.at[peer], got.at[c, y], got_ss, got_rs.at[c], offset, 1)

    def weight(m):
        if m == 1:
            loads[3].wait()
            loads[4].wait()
            column = jnp.broadcast_to(gain_v[1], (LANES, cols)).T[:, :1]
            stage[m] = (up_v[1] * column).astype(BF16)
        else:
            loads[2 if m == 0 else 5].wait()
            stage[m] = down_v[m // 2].astype(BF16)

    def share(m, slot, offsets):
        for offset in offsets:
            send(stage.at[m], wall.at[m, slot], w_ss.at[m], w_rs.at[m], offset, 1)

    def whole(m, c):
        return wall[m, c * NY:(c + 1) * NY].reshape(NY * cols, wall.shape[-1])

    loads[0].start()
    loads[1].start()
    load_u.start()

    @pl.when(core == 1)
    def _():
        for offset in ALONG_Z[:3]:
            signal(barrier, offset, 0)
        for offset in ALONG_Y:
            signal(barrier, offset, 1)
        for offset in ALONG_Z[3:] + ALONG_X:
            signal(barrier, offset, 0)
        for load in loads[2:]:
            load.start()
        first_products()
        got[1, y] = given[y]
        pl.semaphore_wait(barrier, NY)
        signal(go, HERE, 0)

        share_products(1, ALONG_Y)
        for offset in ALONG_Y:
            send(ut.at[y], ut.at[y], u_ss, u_rs, offset, 1)
        for m in range(3):
            weight(m)
            share(m, NY + y, ALONG_Y)
            wall[m, NY + y] = stage[m]

        def send_second(to_z, q, ss):
            @pl.when(z != to_z)
            def _():
                pltpu.make_async_remote_copy(
                    src_ref=pre.at[1, q, z], dst_ref=pre.at[1, q, z],
                    send_sem=ss, recv_sem=pre_rs.at[1, q],
                    device_id={"ra": to_z * NY + y, "cb": x * 2 + 1}, device_id_type=MESH,
                ).start()

        def sent_second(to_z, ss):
            @pl.when(z != to_z)
            def _():
                arrived(pre.at[1, :, 0], ss)

        def share_squares(layer, u):
            sq[layer, z] = jnp.sum((u * u).T, axis=0, keepdims=True)
            for offset in ALONG_Z:
                send(sq.at[layer, z], sq.at[layer, z], sq_ss.at[layer], sq_rs.at[layer], offset, 1)

        floated = None
        wide = pre.shape[-1]
        for layer in range(2):
            for q in range(CHUNKS):
                c, lane = 1 - q // (CHUNKS // 2), q % (CHUNKS // 2) * wide
                if layer == 0 and not lane:
                    arrived(got.at[c, pl.ds(0, NY - c)], got_rs.at[c])
                    part = got[c, 0].astype(F32)
                    for j in range(1, NY):
                        part += got[c, j].astype(F32)
                elif not lane:
                    if c:
                        arrived(wall.at[1, pl.ds(0, 2 * NY - 1)], w_rs.at[1])
                    part = jnp.dot(floated.astype(BF16), whole(1, c), preferred_element_type=F32)
                pre[layer, q, z] = part[:, lane:lane + wide].astype(BF16)
                if layer == 0 and q == 0:
                    pl.semaphore_wait(all_in, 1)
                if layer == 0:
                    for k in FIRST_Z[q]:
                        send(pre.at[0, q, z], pre.at[0, q, z],
                             pre_ss.at[0], pre_rs.at[0, q], (k, 0, 0), 1)
                else:
                    send_second(0, q, first_ss)
                if layer == 1 and q == 0:
                    share_squares(1, floated)
            if layer == 1:
                sent_second(0, first_ss)
                for to_z in LATER_Z:
                    for q in range(CHUNKS):
                        send_second(to_z, q, pre_ss.at[1])
            else:
                arrived(ut.at[pl.ds(0, NY - 1)], u_rs)
                rows_v[...] = ut[...].reshape(NY * cols, tokens).astype(F32).T
                floated = rows_v[pl.ds(pl.multiple_of(y * mine, mine), mine)]
                share_squares(0, floated)
            arrived(wall.at[2 * layer, pl.ds(0, 2 * NY - 1)], w_rs.at[2 * layer])

            def scale_of(layer):
                arrived(sq.at[layer, pl.ds(0, NZ - 1)], sq_rs.at[layer])
                squares = sq[layer, 0]
                for j in range(1, NZ):
                    squares += sq[layer, j]
                factor = 1.0 / (squares / width + EPS)
                return jnp.broadcast_to(factor, (LANES, mine)).T

            total = jnp.zeros((mine, LANES), F32)
            for q in range(CHUNKS):
                c, lane = 1 - q // (CHUNKS // 2), q % (CHUNKS // 2) * wide
                if layer == 1 and q == CHUNKS - 1:
                    scale = scale_of(1)
                arrived(pre.at[layer, q, pl.ds(0, NZ - 1)], pre_rs.at[layer, q])
                preact = pre[layer, q, 0].astype(F32)
                for j in range(1, NZ):
                    preact += pre[layer, q, j].astype(F32)
                positive = jnp.maximum(preact, 0.0)
                act = (positive * positive).astype(BF16)
                total += lax.dot_general(
                    act, whole(2 * layer, c)[:, lane:lane + wide], NT, preferred_element_type=F32)
            if layer == 0:
                branch[x] = total.astype(BF16)
                for offset in ALONG_X:
                    send(branch.at[x], branch.at[x], br_ss, br_rs, offset, 1)
                scale = scale_of(0)

            if layer == 0:
                arrived(branch.at[pl.ds(0, NX - 1)], br_rs)
                total = branch[0].astype(F32)
                for j in range(1, NX):
                    total += branch[j].astype(F32)
                floated = (RESIDUAL * floated + total * scale).astype(BF16).astype(F32)
            else:
                fin[here] = (total * scale + floated * (RESIDUAL / NX)).astype(BF16)
                for offset in PLANE:
                    send(fin.at[here], fin.at[here], fin_ss, fin_rs, offset, 1)
                for offset in PLANE + [HERE]:
                    send(fin.at[here], fin.at[here], fin_ss0, fin_rs, offset, 0)
        arrived(fin.at[pl.ds(0, NX * NY - 1)], fin_rs)

    @pl.when(core == 0)
    def _():
        signal(barrier, HERE, 1)
        for load in loads[2:]:
            load.start()
        first_products()
        pl.semaphore_wait(go, 1)
        share_products(0, ALONG_Y + [HERE])
        weight(0)
        share(0, y, ALONG_Y + [HERE])
        pl.semaphore_wait(barrier, NZ - 1 + NX - 1)
        signal(all_in, HERE, 1)
        for m in (1, 2):
            weight(m)
            share(m, y, ALONG_Y + [HERE])
        arrived(given, got_ss)
        for m in range(3):
            arrived(wall.at[m, pl.ds(0, NY)], w_ss.at[m])
        arrived(fin, fin_rs)

    blocks = []
    for j in range(NY):
        total = fin[j * NX].astype(F32)
        for k in range(1, NX):
            total += fin[j * NX + k].astype(F32)
        blocks.append(total.astype(BF16))
    pick = (
        lax.broadcasted_iota(jnp.int32, (cols, LANES), 1)
        == lax.broadcasted_iota(jnp.int32, (cols, LANES), 0) + y * cols
    ).astype(F32).astype(BF16)
    out_ref[...] = lax.dot_general(
        pick, jnp.concatenate(blocks, axis=0), NT, preferred_element_type=F32).astype(BF16)

    @pl.when(core == 1)
    def _():
        arrived(ut.at[pl.ds(0, NY - 1)], u_ss)
        arrived(given.at[pl.ds(0, NY - 1)], got_ss)
        for m in range(3):
            arrived(wall.at[m, pl.ds(0, NY - 1)], w_ss.at[m])
        arrived(pre.at[0, :, pl.ds(0, NZ - 1)], pre_ss.at[0])
        for to_z in LATER_Z:
            @pl.when(z != to_z)
            def _():
                arrived(pre.at[1, :, 0], pre_ss.at[1])
        for layer in range(2):
            arrived(sq.at[layer, pl.ds(0, NZ - 1)], sq_ss.at[layer])
        arrived(branch.at[pl.ds(0, NX - 1)], br_ss)
        arrived(fin.at[pl.ds(0, NX * NY - 1)], fin_ss)
        arrived(fin, fin_ss0)


def local(stream, gain_first, up_first, down_first, gain_second, up_second, down_second):
    tokens, cols = stream.shape
    hidden = up_first.shape[1]
    mine = tokens // NY
    dma = pltpu.SemaphoreType.DMA
    operands = [
        pltpu.with_memory_space_constraint(a, pltpu.HBM) for a in (
            stream.T, gain_first.reshape(1, cols), up_first, down_first.T,
            gain_second.reshape(1, cols), up_second, down_second.T)
    ]
    out = pl.pallas_call(
        functools.partial(kernel, cols * NZ * NY),
        out_shape=jax.ShapeDtypeStruct((cols, tokens), BF16),
        in_specs=[pl.BlockSpec(memory_space=pl.ANY)] * 7,
        out_specs=pl.BlockSpec(memory_space=pltpu.VMEM),
        scratch_shapes=[
            pltpu.VMEM((2, 1, cols), F32),
            pltpu.VMEM((2, cols, hidden), F32),
            pltpu.VMEM((2, cols, hidden), F32),
            pltpu.VMEM((3, cols, hidden), BF16),
            pltpu.VMEM((3, 2 * NY, cols, hidden), BF16),
            pltpu.VMEM((NY, mine, hidden), BF16),
            pltpu.VMEM((2, NY, mine, hidden), BF16),
            pltpu.VMEM((NY, cols, tokens), BF16),
            pltpu.VMEM((tokens, NY * cols), F32),
            pltpu.VMEM((2, CHUNKS, NZ, mine, 2 * hidden // CHUNKS), BF16),
            pltpu.VMEM((2, NZ, 1, mine), F32),
            pltpu.VMEM((NX, mine, LANES), BF16),
            pltpu.VMEM((NX * NY, mine, LANES), BF16),
            dma((7,)),
            dma((3,)), dma((3,)),
            dma, dma((2,)),
            dma, dma,
            dma((2,)), dma((2, CHUNKS)),
            dma((2,)), dma((2,)),
            dma, dma,
            dma, dma, dma,
            pltpu.SemaphoreType.REGULAR, pltpu.SemaphoreType.REGULAR, dma,
        ],
        compiler_params=pltpu.CompilerParams(
            collective_id=0, has_side_effects=True, vmem_limit_bytes=16 * 1024 * 1024,
        ),
    )(*operands)
    return out.T


def solution(mesh):
    return jax.shard_map(
        local,
        mesh=mesh,
        in_specs=(
            P(None, "ra"),
            P("ra"),
            P("ra", "cb"),
            P("cb", "ra"),
            P("ra"),
            P("ra", "cb"),
            P("cb", "ra"),
        ),
        out_specs=P(None, "ra"),
        check_vma=False,
    )
```

```python
import functools

import jax
import jax.numpy as jnp
from jax import lax
from jax.experimental import pallas as pl
from jax.experimental.pallas import tpu as pltpu
from jax.sharding import PartitionSpec as P

NZ, NY, NX = 8, 4, 4
CHUNKS = 4
EPS = 1e-06
RESIDUAL = 0.25
LANES = 128
MESH = pl.DeviceIdType.MESH
F32 = jnp.float32
BF16 = jnp.bfloat16
NT = (((1,), (1,)), ((), ()))


def ring(offset, size):
    return min(offset, size - offset)


def farthest_first(offsets):
    return sorted(
        offsets, key=lambda o: (-(ring(o[0], NZ) + ring(o[1], NY) + ring(o[2], NX)), o))


ALONG_Y = farthest_first([(0, k, 0) for k in range(1, NY)])
ALONG_X = farthest_first([(0, 0, k) for k in range(1, NX)])
ALONG_Z = farthest_first([(k, 0, 0) for k in range(1, NZ)])
FIRST_Z = [[4, 3, 5, 2, 6, 1, 7], [3, 5, 2, 4, 6, 1, 7], [4, 5, 3, 2, 6, 1, 7], [4, 3, 5, 2, 6, 1, 7]]
LATER_Z = [1, 2, 7, 6, 3, 4, 5]
PLANE = farthest_first([(0, j, k) for j in range(NY) for k in range(NX) if j or k])
HERE = (0, 0, 0)


def kernel(
    width,
    stream_hbm, gain1_hbm, up1_hbm, down1_hbm, gain2_hbm, up2_hbm, down2_hbm,
    out_ref,
    gain_v, up_v, down_v, stage, wall, given, got, ut, rows_v, pre, sq, branch, fin,
    load_sem, w_ss, w_rs, got_ss, got_rs, u_ss, u_rs, pre_ss, pre_rs, sq_ss, sq_rs,
    br_ss, br_rs, fin_ss, fin_rs, fin_ss0, go, all_in, first_ss,
):
    ra = lax.axis_index("ra")
    cb = lax.axis_index("cb")
    z, y = lax.div(ra, NY), lax.rem(ra, NY)
    x, core = lax.div(cb, 2), lax.rem(cb, 2)
    here = y * NX + x
    cols, tokens = ut.shape[1:]
    mine = tokens // NY

    def device(offset, at_core):
        dz, dy, dx = offset
        to_z = lax.rem(z + dz, NZ) if dz else z
        to_y = lax.rem(y + dy, NY) if dy else y
        to_x = lax.rem(x + dx, NX) if dx else x
        return {"ra": to_z * NY + to_y, "cb": to_x * 2 + at_core}

    def send(src, dst, ss, rs, offset, at_core):
        pltpu.make_async_remote_copy(
            src_ref=src, dst_ref=dst, send_sem=ss, recv_sem=rs,
            device_id=device(offset, at_core), device_id_type=MESH,
        ).start()

    def arrived(ref, rs):
        pltpu.make_async_copy(ref, ref, rs).wait()

    def signal(sem, offset, at_core):
        pl.semaphore_signal(
            sem, inc=1, device_id=device(offset, at_core), device_id_type=MESH)

    loads = [
        pltpu.make_async_copy(src, dst, load_sem.at[i])
        for i, (src, dst) in enumerate((
            (gain1_hbm, gain_v.at[0]),
            (up1_hbm, up_v.at[0]),
            (down1_hbm, down_v.at[0]),
            (gain2_hbm, gain_v.at[1]),
            (up2_hbm, up_v.at[1]),
            (down2_hbm, down_v.at[1]),
        ))
    ]
    load_u = pltpu.make_async_copy(stream_hbm, ut.at[y], load_sem.at[6])
    barrier = pltpu.get_barrier_semaphore()

    def first_products():
        load_u.wait()
        loads[0].wait()
        scaled = (ut[y].astype(F32).T * gain_v[0]).astype(BF16)
        loads[1].wait()
        part = jnp.dot(scaled, up_v[0].astype(BF16), preferred_element_type=F32).astype(BF16)
        for j in range(NY):
            given[j] = part[j * mine:(j + 1) * mine]

    def share_products(c, offsets):
        for offset in offsets:
            peer = lax.rem(y + offset[1], NY)
            send(given.at[peer], got.at[c, y], got_ss, got_rs.at[c], offset, 1)

    def weight(m):
        if m == 1:
            loads[3].wait()
            loads[4].wait()
            column = jnp.broadcast_to(gain_v[1], (LANES, cols)).T[:, :1]
            stage[m] = (up_v[1] * column).astype(BF16)
        else:
            loads[2 if m == 0 else 5].wait()
            stage[m] = down_v[m // 2].astype(BF16)

    def share(m, slot, offsets):
        for offset in offsets:
            send(stage.at[m], wall.at[m, slot], w_ss.at[m], w_rs.at[m], offset, 1)

    def whole(m, c):
        return wall[m, c * NY:(c + 1) * NY].reshape(NY * cols, wall.shape[-1])

    @pl.when(core == 1)
    def _():
        for offset in ALONG_Z[:3]:
            signal(barrier, offset, 0)

    loads[0].start()
    loads[1].start()
    load_u.start()

    @pl.when(core == 1)
    def _():
        for offset in ALONG_Y:
            signal(barrier, offset, 1)
        for offset in ALONG_Z[3:] + ALONG_X:
            signal(barrier, offset, 0)
        for load in loads[2:]:
            load.start()
        first_products()
        got[1, y] = given[y]
        pl.semaphore_wait(barrier, NY)
        signal(go, HERE, 0)

        share_products(1, ALONG_Y)
        for offset in ALONG_Y:
            send(ut.at[y], ut.at[y], u_ss, u_rs, offset, 1)
        for m in range(3):
            weight(m)
            share(m, NY + y, ALONG_Y)
            wall[m, NY + y] = stage[m]

        def send_second(to_z, q, ss):
            @pl.when(z != to_z)
            def _():
                pltpu.make_async_remote_copy(
                    src_ref=pre.at[1, q, z], dst_ref=pre.at[1, q, z],
                    send_sem=ss, recv_sem=pre_rs.at[1, q],
                    device_id={"ra": to_z * NY + y, "cb": x * 2 + 1}, device_id_type=MESH,
                ).start()

        def sent_second(to_z, ss):
            @pl.when(z != to_z)
            def _():
                arrived(pre.at[1, :, 0], ss)

        def share_squares(layer, u):
            sq[layer, z] = jnp.sum((u * u).T, axis=0, keepdims=True)
            for offset in ALONG_Z:
                send(sq.at[layer, z], sq.at[layer, z], sq_ss.at[layer], sq_rs.at[layer], offset, 1)

        floated = None
        wide = pre.shape[-1]
        for layer in range(2):
            for q in range(CHUNKS):
                c, lane = 1 - q // (CHUNKS // 2), q % (CHUNKS // 2) * wide
                if layer == 0 and not lane:
                    arrived(got.at[c, pl.ds(0, NY - c)], got_rs.at[c])
                    part = got[c, 0].astype(F32)
                    for j in range(1, NY):
                        part += got[c, j].astype(F32)
                elif not lane:
                    if c:
                        arrived(wall.at[1, pl.ds(0, 2 * NY - 1)], w_rs.at[1])
                    part = jnp.dot(floated.astype(BF16), whole(1, c), preferred_element_type=F32)
                pre[layer, q, z] = part[:, lane:lane + wide].astype(BF16)
                if layer == 0 and q == 0:
                    pl.semaphore_wait(all_in, 1)
                if layer == 0:
                    for k in FIRST_Z[q]:
                        send(pre.at[0, q, z], pre.at[0, q, z],
                             pre_ss.at[0], pre_rs.at[0, q], (k, 0, 0), 1)
                else:
                    send_second(0, q, first_ss)
                if layer == 1 and q == 0:
                    share_squares(1, floated)
            if layer == 1:
                sent_second(0, first_ss)
                for to_z in LATER_Z:
                    for q in range(CHUNKS):
                        send_second(to_z, q, pre_ss.at[1])
            else:
                arrived(ut.at[pl.ds(0, NY - 1)], u_rs)
                rows_v[...] = ut[...].reshape(NY * cols, tokens).astype(F32).T
                floated = rows_v[pl.ds(pl.multiple_of(y * mine, mine), mine)]
                share_squares(0, floated)
            arrived(wall.at[2 * layer, pl.ds(0, 2 * NY - 1)], w_rs.at[2 * layer])

            def scale_of(layer):
                arrived(sq.at[layer, pl.ds(0, NZ - 1)], sq_rs.at[layer])
                squares = sq[layer, 0]
                for j in range(1, NZ):
                    squares += sq[layer, j]
                factor = 1.0 / (squares / width + EPS)
                return jnp.broadcast_to(factor, (LANES, mine)).T

            total = jnp.zeros((mine, LANES), F32)
            for q in range(CHUNKS):
                c, lane = 1 - q // (CHUNKS // 2), q % (CHUNKS // 2) * wide
                if layer == 1 and q == CHUNKS - 1:
                    scale = scale_of(1)
                arrived(pre.at[layer, q, pl.ds(0, NZ - 1)], pre_rs.at[layer, q])
                preact = pre[layer, q, 0].astype(F32)
                for j in range(1, NZ):
                    preact += pre[layer, q, j].astype(F32)
                positive = jnp.maximum(preact, 0.0)
                act = (positive * positive).astype(BF16)
                total += lax.dot_general(
                    act, whole(2 * layer, c)[:, lane:lane + wide], NT, preferred_element_type=F32)
            if layer == 0:
                branch[x] = total.astype(BF16)
                for offset in ALONG_X:
                    send(branch.at[x], branch.at[x], br_ss, br_rs, offset, 1)
                scale = scale_of(0)

            if layer == 0:
                arrived(branch.at[pl.ds(0, NX - 1)], br_rs)
                total = branch[0].astype(F32)
                for j in range(1, NX):
                    total += branch[j].astype(F32)
                floated = (RESIDUAL * floated + total * scale).astype(BF16).astype(F32)
            else:
                fin[here] = (total * scale + floated * (RESIDUAL / NX)).astype(BF16)
                for offset in PLANE:
                    send(fin.at[here], fin.at[here], fin_ss, fin_rs, offset, 1)
                for offset in PLANE + [HERE]:
                    send(fin.at[here], fin.at[here], fin_ss0, fin_rs, offset, 0)
        arrived(fin.at[pl.ds(0, NX * NY - 1)], fin_rs)

    @pl.when(core == 0)
    def _():
        signal(barrier, HERE, 1)
        for load in loads[2:]:
            load.start()
        first_products()
        pl.semaphore_wait(go, 1)
        share_products(0, ALONG_Y + [HERE])
        pl.semaphore_wait(barrier, NZ - 1 + NX - 1)
        signal(all_in, HERE, 1)
        for m in range(3):
            weight(m)
            share(m, y, ALONG_Y + [HERE])
        arrived(given, got_ss)
        for m in range(3):
            arrived(wall.at[m, pl.ds(0, NY)], w_ss.at[m])
        arrived(fin, fin_rs)

    blocks = []
    for j in range(NY):
        total = fin[j * NX].astype(F32)
        for k in range(1, NX):
            total += fin[j * NX + k].astype(F32)
        blocks.append(total.astype(BF16))
    pick = (
        lax.broadcasted_iota(jnp.int32, (cols, LANES), 1)
        == lax.broadcasted_iota(jnp.int32, (cols, LANES), 0) + y * cols
    ).astype(F32).astype(BF16)
    out_ref[...] = lax.dot_general(
        pick, jnp.concatenate(blocks, axis=0), NT, preferred_element_type=F32).astype(BF16)

    @pl.when(core == 1)
    def _():
        arrived(ut.at[pl.ds(0, NY - 1)], u_ss)
        arrived(given.at[pl.ds(0, NY - 1)], got_ss)
        for m in range(3):
            arrived(wall.at[m, pl.ds(0, NY - 1)], w_ss.at[m])
        arrived(pre.at[0, :, pl.ds(0, NZ - 1)], pre_ss.at[0])
        for to_z in LATER_Z:
            @pl.when(z != to_z)
            def _():
                arrived(pre.at[1, :, 0], pre_ss.at[1])
        for layer in range(2):
            arrived(sq.at[layer, pl.ds(0, NZ - 1)], sq_ss.at[layer])
        arrived(branch.at[pl.ds(0, NX - 1)], br_ss)
        arrived(fin.at[pl.ds(0, NX * NY - 1)], fin_ss)
        arrived(fin, fin_ss0)


def local(stream, gain_first, up_first, down_first, gain_second, up_second, down_second):
    tokens, cols = stream.shape
    hidden = up_first.shape[1]
    mine = tokens // NY
    dma = pltpu.SemaphoreType.DMA
    operands = [
        pltpu.with_memory_space_constraint(a, pltpu.HBM) for a in (
            stream.T, gain_first.reshape(1, cols), up_first, down_first.T,
            gain_second.reshape(1, cols), up_second, down_second.T)
    ]
    out = pl.pallas_call(
        functools.partial(kernel, cols * NZ * NY),
        out_shape=jax.ShapeDtypeStruct((cols, tokens), BF16),
        in_specs=[pl.BlockSpec(memory_space=pl.ANY)] * 7,
        out_specs=pl.BlockSpec(memory_space=pltpu.VMEM),
        scratch_shapes=[
            pltpu.VMEM((2, 1, cols), F32),
            pltpu.VMEM((2, cols, hidden), F32),
            pltpu.VMEM((2, cols, hidden), F32),
            pltpu.VMEM((3, cols, hidden), BF16),
            pltpu.VMEM((3, 2 * NY, cols, hidden), BF16),
            pltpu.VMEM((NY, mine, hidden), BF16),
            pltpu.VMEM((2, NY, mine, hidden), BF16),
            pltpu.VMEM((NY, cols, tokens), BF16),
            pltpu.VMEM((tokens, NY * cols), F32),
            pltpu.VMEM((2, CHUNKS, NZ, mine, 2 * hidden // CHUNKS), BF16),
            pltpu.VMEM((2, NZ, 1, mine), F32),
            pltpu.VMEM((NX, mine, LANES), BF16),
            pltpu.VMEM((NX * NY, mine, LANES), BF16),
            dma((7,)),
            dma((3,)), dma((3,)),
            dma, dma((2,)),
            dma, dma,
            dma((2,)), dma((2, CHUNKS)),
            dma((2,)), dma((2,)),
            dma, dma,
            dma, dma, dma,
            pltpu.SemaphoreType.REGULAR, pltpu.SemaphoreType.REGULAR, dma,
        ],
        compiler_params=pltpu.CompilerParams(
            collective_id=0, has_side_effects=True, vmem_limit_bytes=16 * 1024 * 1024,
        ),
    )(*operands)
    return out.T


def solution(mesh):
    return jax.shard_map(
        local,
        mesh=mesh,
        in_specs=(
            P(None, "ra"),
            P("ra"),
            P("ra", "cb"),
            P("cb", "ra"),
            P("ra"),
            P("ra", "cb"),
            P("cb", "ra"),
        ),
        out_specs=P(None, "ra"),
        check_vma=False,
    )
```
